256 devices in a mesh: sp: 32 (over z, y), dp: 8 (over x, core).
Axes of the slice: x: 4, y: 4, z: 8, core: 2. Of those that a mesh axis runs over, the one named last changes fastest.
Arguments:
- cotangent: bfloat16 [8, 8192, 4096], P('dp', 'sp'), may hold values from -6 to 6
- up_pre: bfloat16 [8, 8192, 4096], P('dp', 'sp'), may hold values from -6 to 6
- value_pre: bfloat16 [8, 8192, 4096], P('dp', 'sp'), may hold values from -6 to 6
- spatial_weight: bfloat16 [32, 1024, 1024], P('sp', 'dp'), may hold values from -0.1875 to 0.1875
- spatial_bias: float32 [32, 1024], P('sp'), may hold values from 0.5 to 1.5
- value_gain: float32 [4096], replicated, may hold values from 0.1 to 1.9
Outputs:
- up_grad: bfloat16 [8, 8192, 4096], P('dp', 'sp')
- value_grad: bfloat16 [8, 8192, 4096], P('dp', 'sp')
- weight_grad: float32 [32, 1024, 1024], P('sp', 'dp')
- bias_grad: float32 [32, 1024], P('sp', 'dp')
- gain_grad: float32 [4096], replicated
The draws below stay inside these ranges and needn't reach their ends.
All inputs are finite; a program needn't handle non-finite values.
Results may differ from the reference program's by a relative error of at most 0.0064.
Values may be sent and summed in bfloat16 or wider, within the bound.
A program may use at most 128 MiB of HBM per device.

```python
import math
import jax
import jax.numpy as jnp
from jax import lax

GROUPS = 32
GROUP = 128
BLOCK = 1024
WIDTH = 4096
SEQ = 8192
BATCH = 8


def shard_levels(key, shape, pieces, least, high):
    gain = 1.0
    for axis_at, parts in pieces:
        draws = jax.random.uniform(jax.random.fold_in(jax.random.fold_in(key, 6), axis_at), (parts,), jnp.float32, least / len(pieces), high / len(pieces))
        gain = gain * jnp.repeat(jnp.exp(draws), shape[axis_at] // parts).reshape((-1,) + (1,) * (len(shape) - 1 - axis_at))
    return gain


def centred(rng, dims, spread, most, pieces=(), dtype=jnp.bfloat16):
    values = jax.random.normal(rng, dims, jnp.float32) * spread
    if len(pieces) > 0:
        values = shard_levels(rng, dims, pieces, -0.22, 0.18) * values
    return jnp.clip(values, min=-most, max=most).astype(dtype)


def setup_inputs(seed: int = 0) -> dict:
    streams_of = jax.random.split(jax.random.key(seed), 7)
    return {
        "cotangent": centred(streams_of[0], (BATCH, SEQ, WIDTH), 1.0, 6.0, ((0, 8), (1, 32))),
        "up_pre": centred(streams_of[1], (BATCH, SEQ, WIDTH), 1.0, 6.0, ((0, 8), (1, 32))),
        "value_pre": centred(streams_of[2], (BATCH, SEQ, WIDTH), 1.0, 6.0, ((0, 8), (1, 32))),
        "spatial_weight": centred(streams_of[3], (GROUPS, BLOCK, BLOCK), BLOCK ** -0.5, 0.1875, ((0, 32), (1, 8))),
        "spatial_bias": jnp.clip(0.5 + 1.0 * jax.random.uniform(streams_of[4], (GROUPS, BLOCK), jnp.float32) ** shard_levels(streams_of[4], (GROUPS, BLOCK), ((0, 32),), -0.2, 0.2), 0.5, 1.5),
        "value_gain": jnp.clip(1.0 + 0.18 * jax.random.normal(streams_of[5], (WIDTH,), jnp.float32), 0.1, 1.9),
    }


norm_floor = 0.5
root_half = 1.0 / math.sqrt(2.0)
inv_root_tau = 1.0 / math.sqrt(2.0 * math.pi)

def gelu_slope(values):
    return 0.5 * (1.0 + jax.scipy.special.erf(values * root_half)) + values * jnp.exp(-0.5 * values * values) * inv_root_tau

def reference(cotangent, up_pre, value_pre, spatial_weight, spatial_bias, value_gain):
    weight_full = spatial_weight.astype(jnp.float32)
    bias_full = spatial_bias.astype(jnp.float32).T[None, :, :, None]
    gain_full = value_gain.astype(jnp.float32)
    block_shape = (SEQ // BLOCK, BLOCK, GROUPS, GROUP)

    def one_sequence(carried, inputs):
        grad_seq, up_seq, value_seq = inputs
        grad_tok = grad_seq.astype(jnp.float32)
        up_arg = up_seq.astype(jnp.float32)
        value_arg = value_seq.astype(jnp.float32)
        up_act = lax.optimization_barrier(jax.nn.gelu(up_arg, approximate=False).astype(jnp.bfloat16))
        value_act = jax.nn.gelu(value_arg, approximate=False)
        inv_rms = lax.rsqrt(lax.optimization_barrier(jnp.mean(value_act * value_act, axis=-1, keepdims=True)) + norm_floor)
        normed = value_act * inv_rms
        value_norm = lax.optimization_barrier((normed * gain_full).astype(jnp.bfloat16))
        gate_tok = lax.optimization_barrier((grad_tok * up_act.astype(jnp.float32)).astype(jnp.bfloat16))
        value_blocks = value_norm.astype(jnp.float32).reshape(block_shape)
        gate_blocks = gate_tok.astype(jnp.float32).reshape(block_shape)
        mixed_out = jnp.einsum('gpq,nqgc->npgc', weight_full, value_blocks) + bias_full
        mixed_out = lax.optimization_barrier(mixed_out.astype(jnp.bfloat16).reshape(SEQ, WIDTH))
        back_seq = jnp.einsum('gpq,npgc->nqgc', weight_full, gate_blocks)
        back_seq = lax.optimization_barrier(back_seq.astype(jnp.bfloat16).reshape(SEQ, WIDTH))
        weight_acc = carried[0] + jnp.einsum('npgc,nqgc->gpq', gate_blocks, value_blocks)
        bias_acc = carried[1] + lax.optimization_barrier(jnp.sum(gate_blocks, axis=(0, 3))).T
        up_mid = lax.optimization_barrier((grad_tok * mixed_out.astype(jnp.float32)).astype(jnp.bfloat16))
        up_out = (up_mid.astype(jnp.float32) * gelu_slope(up_arg)).astype(jnp.bfloat16)
        back_full = back_seq.astype(jnp.float32)
        gain_acc = carried[2] + lax.optimization_barrier(jnp.sum(back_full * normed, axis=0))
        scaled = back_full * gain_full
        value_slope = inv_rms * scaled - inv_rms ** 3 * value_act * lax.optimization_barrier(jnp.mean(scaled * value_act, axis=-1, keepdims=True))
        value_out = (value_slope * gelu_slope(value_arg)).astype(jnp.bfloat16)
        return ((weight_acc, bias_acc, gain_acc), (up_out, value_out))
    initial = (jnp.zeros((GROUPS, BLOCK, BLOCK), jnp.float32), jnp.zeros((GROUPS, BLOCK), jnp.float32), jnp.zeros((WIDTH,), jnp.float32))
    totals, outputs = lax.scan(one_sequence, initial, (cotangent, up_pre, value_pre))
    return (outputs[0], outputs[1], totals[0], totals[1], totals[2])
```

```python
import math

import jax
import jax.numpy as jnp
from jax import lax
from jax.sharding import Mesh
from jax.sharding import PartitionSpec as P

SP = ("sp_0", "sp_1")
DP = ("dp_0", "dp_1")
PLANE = ("dp_0", "dp_1", "sp_1")
SWAP = ("sp_0", "dp_0", "dp_1")
ALL = ("sp_0", "sp_1", "dp_0", "dp_1")


norm_floor = 0.5
root_half = 1.0 / math.sqrt(2.0)
inv_root_tau = 1.0 / math.sqrt(2.0 * math.pi)


def gelu_slope(values):
    return (
        0.5 * (1.0 + jax.scipy.special.erf(values * root_half))
        + values * jnp.exp(-0.5 * values * values) * inv_root_tau
    )


def swapped(shard, n):
    pairs = [(a * n + b, b * n + a) for a in range(n) for b in range(n)]
    return lax.ppermute(shard, SWAP, pairs)


def shards(cotangent, up_pre, value_pre, spatial_weight, spatial_bias, value_gain):
    rows, width = cotangent.shape[1:]
    block_len = spatial_weight.shape[2]
    planes = lax.axis_size("sp_0")
    seqs = lax.axis_size(DP)
    groups = lax.axis_size(PLANE)
    dim = width // groups
    weight = lax.all_gather(swapped(spatial_weight[0], planes), "sp_0", axis=0, tiled=True)
    bias = swapped(spatial_bias, planes)[0]

    grad_tok = cotangent[0].astype(jnp.float32)
    up_arg = up_pre[0].astype(jnp.float32)
    value_arg = value_pre[0].astype(jnp.float32)
    up_act = lax.optimization_barrier(jax.nn.gelu(up_arg, approximate=False).astype(jnp.bfloat16))
    value_act = jax.nn.gelu(value_arg, approximate=False)
    inv_rms = lax.rsqrt(jnp.mean(value_act * value_act, axis=-1, keepdims=True) + norm_floor)
    normed = value_act * inv_rms
    value_norm = (normed * value_gain).astype(jnp.bfloat16)
    gate_tok = (grad_tok * up_act.astype(jnp.float32)).astype(jnp.bfloat16)

    def outward(tok):
        tok = tok.reshape(rows, groups, dim).transpose(1, 0, 2)
        got = lax.all_to_all(tok, PLANE, split_axis=0, concat_axis=0, tiled=True)
        return got.reshape(seqs, block_len, dim)

    def homeward(heads):
        got = heads.reshape(groups, rows, dim)
        got = lax.all_to_all(got, PLANE, split_axis=0, concat_axis=0, tiled=True)
        return got.transpose(1, 0, 2).reshape(rows, width)

    value_blocks = outward(value_norm)
    gate_blocks = outward(gate_tok)
    back_heads = jnp.einsum(
        "pq,npc->nqc", weight, gate_blocks, preferred_element_type=jnp.float32
    ).astype(jnp.bfloat16)
    back_full = homeward(back_heads).astype(jnp.float32)
    mixed_heads = jnp.einsum("pq,nqc->npc", weight, value_blocks, preferred_element_type=jnp.float32)
    mixed_heads = (mixed_heads + bias[None, :, None]).astype(jnp.bfloat16)
    mixed_tok = homeward(mixed_heads).astype(jnp.float32)
    weight_term = jnp.einsum(
        "npc,nqc->pq", gate_blocks, value_blocks, preferred_element_type=jnp.float32
    )
    bias_term = jnp.sum(gate_blocks, axis=(0, 2), dtype=jnp.float32)
    both = jnp.concatenate([weight_term, jnp.broadcast_to(bias_term[:, None], (block_len, 128))], axis=1)
    both = lax.psum_scatter(both, "sp_0", scatter_dimension=0, tiled=True)
    both = swapped(both, planes)
    weight_grad = both[None, :, :block_len]
    bias_grad = both[None, :, block_len]

    up_mid = lax.optimization_barrier((grad_tok * mixed_tok).astype(jnp.bfloat16))
    up_grad = (up_mid.astype(jnp.float32) * gelu_slope(up_arg)).astype(jnp.bfloat16)[None]
    gain_grad = lax.psum(jnp.sum(back_full * normed, axis=0), ALL)
    scaled = back_full * value_gain
    value_slope = inv_rms * scaled - inv_rms**3 * value_act * jnp.mean(
        scaled * value_act, axis=-1, keepdims=True
    )
    value_grad = (value_slope * gelu_slope(value_arg)).astype(jnp.bfloat16)[None]
    return (up_grad, value_grad, weight_grad, bias_grad, gain_grad)


def solution(mesh):
    torus = Mesh(mesh.devices.reshape(8, 4, 4, 2), ("sp_0", "sp_1", "dp_0", "dp_1"))
    in_specs = (
        P(DP, SP, None),
        P(DP, SP, None),
        P(DP, SP, None),
        P(SP, DP, None),
        P(SP, None),
        P(),
    )
    out_specs = (P(DP, SP, None), P(DP, SP, None), P(SP, DP, None), P(SP, DP), P())
    return jax.shard_map(
        shards, mesh=torus, in_specs=in_specs, out_specs=out_specs, check_vma=False
    )
```

```python
import math

import jax
import jax.numpy as jnp
from jax import lax
from jax.experimental import pallas as pl
from jax.experimental.pallas import tpu as pltpu
from jax.sharding import Mesh
from jax.sharding import PartitionSpec as P

SP = ("sp_0", "sp_1")
DP = ("dp_0", "dp_1")

NZ, NY, NX, NC = 8, 4, 4, 2
NI = NX * NC
ROWS = 256
DIM = 128
WIDTH = NI * NY * DIM
CHUNK = NY * DIM
BLOCK = NY * ROWS
PART = BLOCK // NZ
F32, BF16 = jnp.float32, jnp.bfloat16

norm_floor = 0.5
root_half = 1.0 / math.sqrt(2.0)
inv_root_tau = 1.0 / math.sqrt(2.0 * math.pi)

ORDER = ((0, 0), (0, 1), (1, 0), (3, 0), (1, 1), (3, 1), (2, 0), (2, 1))
NT = (((1,), (1,)), ((), ()))


def phi(x):
    return 0.5 * (1.0 + lax.erf(x * root_half))


def slope(x):
    return phi(x) + x * jnp.exp(-0.5 * x * x) * inv_root_tau


def kernel(
    cot_hbm, up_hbm, val_hbm, w_hbm, bias_hbm, gain_hbm,
    upg_hbm, valg_hbm, wg_hbm, bg_hbm, gg_hbm,
    cot, up, val, w_own, b_own, gain,
    S, X, Y, R, H, B,
    w_in, b_in, W, WT, bcol,
    wga, ws, wr, wsum, wout, bsend, br, bsum, bout,
    gsend, gz, gxs, gx, gys, gy,
    act, su, sv, inv, dot, gacc,
    in_sem, out_sem,
    xo_send, xo_recv, yo_send, yo_recv,
    sw_send, sw_recv, wz_send, wz_recv,
    yr_send, yr_recv, xr_send, xr_recv,
    gr_send, gr_recv, so_send, so_recv,
    gn_send, gn_recv,
):
    z, y, x, c = (lax.axis_index(a) for a in ("sp_0", "sp_1", "dp_0", "dp_1"))
    me = x * NC + c

    def remote(src, dst, send, recv, where):
        return pltpu.make_async_remote_copy(
            src_ref=src, dst_ref=dst, send_sem=send, recv_sem=recv,
            device_id=where, device_id_type=pl.DeviceIdType.MESH,
        )

    def at_xc(dx, dc):
        return lax.rem(x + dx, NX), lax.rem(c + dc, NC)

    def from_xc(dx, dc):
        return lax.rem(x + NX - dx, NX), lax.rem(c + NC - dc, NC)

    def wait(ref, sem):
        pltpu.make_async_copy(ref, ref, sem).wait()

    loads = [
        pltpu.make_async_copy(src, dst, in_sem.at[k])
        for k, (src, dst) in enumerate(
            ((up_hbm, up), (cot_hbm, cot), (w_hbm, w_own), (bias_hbm, b_own), (val_hbm, val), (gain_hbm, gain))
        )
    ]
    for load in loads:
        load.start()

    barrier = pltpu.get_barrier_semaphore()

    def greet(where):
        pl.semaphore_signal(barrier, inc=1, device_id=where, device_id_type=pl.DeviceIdType.MESH)

    for dx, dc in ORDER[1:]:
        xi, ci = at_xc(dx, dc)
        greet({"dp_0": xi, "dp_1": ci})
    for dy in range(1, NY):
        greet({"sp_1": lax.rem(y + dy, NY)})
    for dz in range(1, NZ):
        greet({"sp_0": lax.rem(z + dz, NZ)})
    swap_to = {"sp_0": me, "dp_0": z // NC, "dp_1": lax.rem(z, NC)}

    @pl.when(me != z)
    def _():
        greet(swap_to)

    peers = NI - 1 + NY - 1 + NZ - 1

    @pl.when(me != z)
    def _():
        pl.semaphore_wait(barrier, peers + 1)

    @pl.when(me == z)
    def _():
        pl.semaphore_wait(barrier, peers)

    loads[2].wait()
    loads[3].wait()
    moves = ((w_own, w_in), (b_own, b_in))

    @pl.when(me != z)
    def _():
        for k, (src, dst) in enumerate(moves):
            remote(src, dst, sw_send.at[k], sw_recv.at[k], swap_to).start()

    @pl.when(me == z)
    def _():
        for k, (src, dst) in enumerate(moves):
            pltpu.make_async_copy(src, dst, sw_recv.at[k]).start()

    def cols(i):
        return pl.ds(pl.multiple_of(i * CHUNK, CHUNK), CHUNK)

    def gate_chunk(i):
        @pl.loop(0, ROWS // 32)
        def _(t):
            rows = pl.ds(pl.multiple_of(t * 32, 32), 32)
            u = up[rows, cols(i)].astype(F32)
            u = (u * phi(u)).astype(BF16).astype(F32)
            g = (cot[rows, cols(i)].astype(F32) * u).astype(BF16)
            for k in range(NY):
                S[0, i, k, rows, :] = g[:, k * DIM : (k + 1) * DIM]

    def slot(xs, cs, row):
        return (
            xs,
            pl.ds(pl.multiple_of(row * ROWS, ROWS), ROWS),
            pl.ds(pl.multiple_of(cs * DIM, DIM), DIM),
        )

    def forward(a, buf, n, d):
        xs, cs = from_xc(*d)
        s = xs * NC + cs
        for dy in range(1, NY):
            to = lax.rem(y + dy, NY)
            remote(
                buf.at[a, s, to], Y.at[(a, *slot(xs, cs, y))],
                yo_send, yo_recv.at[a, d[0]], {"sp_1": to},
            ).start()
        pltpu.make_async_copy(buf.at[a, s, y], Y.at[(a, *slot(xs, cs, y))], yo_recv.at[a, d[0]]).start()

    def push(a, n):
        d = ORDER[n]
        if n == 0:
            forward(a, S, n, d)
            return
        xi, ci = at_xc(*d)
        remote(
            S.at[a, xi * NC + ci], X.at[a, me], xo_send, xo_recv.at[a, n], {"dp_0": xi, "dp_1": ci}
        ).start()

    def relay(a, n):
        xs, cs = from_xc(*ORDER[n])
        wait(X.at[a, xs * NC + cs], xo_recv.at[a, n])
        forward(a, X, n, ORDER[n])

    loads[0].wait()
    loads[1].wait()
    for n, d in enumerate(ORDER):
        xi, ci = at_xc(*d)
        gate_chunk(xi * NC + ci)
        if n > 0:
            push(0, n - 1)
    loads[4].wait()
    loads[5].wait()

    wait(w_in, sw_recv.at[0])
    wait(b_in, sw_recv.at[1])
    push(0, NI - 1)
    for dz in range(1, NZ):
        remote(w_in, W.at[z], wz_send, wz_recv, {"sp_0": lax.rem(z + dz, NZ)}).start()
    pltpu.make_async_copy(w_in, W.at[z], wz_recv).start()

    @pl.loop(0, ROWS // 16)
    def _(t):
        rows = pl.ds(pl.multiple_of(t * 16, 16), 16)
        total = jnp.zeros((16, DIM), F32)
        for i in range(NI):
            v = val[rows, i * CHUNK : (i + 1) * CHUNK].astype(F32)
            v = v * phi(v)
            act[rows, i * CHUNK : (i + 1) * CHUNK] = v
            v = v * v
            for k in range(NY):
                total += v[:, k * DIM : (k + 1) * DIM]
        scale = lax.rsqrt(jnp.sum(total, axis=1, keepdims=True) / WIDTH + norm_floor)
        inv[rows, :] = jnp.broadcast_to(scale, (16, DIM))
        for i in range(NI):
            for k in range(NY):
                at = slice((i * NY + k) * DIM, (i * NY + k + 1) * DIM)
                S[1, i, k, rows, :] = (act[rows, at] * scale * gain[0:1, at]).astype(BF16)

    for n in range(2, NI):
        push(1, n)
    push(1, 1)
    push(1, 0)

    def slopes(src, dst):
        @pl.loop(0, ROWS // 32 * NI)
        def _(t):
            rows = pl.ds(pl.multiple_of(t // NI * 32, 32), 32)
            at = cols(lax.rem(t, NI))
            dst[rows, at] = slope(src[rows, at].astype(F32))

    for n in range(1, 6):
        relay(0, n)
    slopes(up, su)
    relay(1, 1)
    for n in (6, 7):
        relay(0, n)
    slopes(val, sv)
    for n in range(2, 6):
        relay(1, n)

    for k in range(BLOCK // DIM):
        part = jnp.broadcast_to(b_in[0:1, k * DIM : (k + 1) * DIM], (DIM, DIM))
        bcol[k * DIM : (k + 1) * DIM, :] = jnp.transpose(part)

    def pair(dx):
        return lax.rem(x + NX - dx, NX)

    for dx in (0, 1, 3):
        for a in range(2):
            wait(Y.at[a, pair(dx)], yo_recv.at[a, dx])

    def tile(t):
        return pl.ds(pl.multiple_of(t * ROWS, ROWS), ROWS)

    def outer(p, i, j):
        return lax.dot_general(Y[0, p, tile(i), :], Y[1, p, tile(j), :], NT, preferred_element_type=F32)

    @pl.loop(0, NY * NY)
    def _(t):
        i, j = t // NY, lax.rem(t, NY)
        wga[tile(i), tile(j)] = outer(pair(0), i, j) + outer(pair(1), i, j) + outer(pair(3), i, j)

    ones = jnp.ones((8, NC * DIM), BF16)

    def row_sums(dx):
        return lax.dot_general(ones, Y[0, pair(dx)], NT, preferred_element_type=F32)

    bsum[...] = row_sums(0) + row_sums(1) + row_sums(3)

    for n in (6, 7):
        relay(1, n)
    wait(W, wz_recv)

    @pl.loop(0, NZ)
    def _(j):
        WT[:, pl.ds(pl.multiple_of(j * PART, PART), PART)] = jnp.transpose(W[j])

    for a in range(2):
        wait(Y.at[a, pair(2)], yo_recv.at[a, 2])

    @pl.loop(0, NY * NY)
    def _(t):
        i, j = t // NY, lax.rem(t, NY)
        total = (wga[tile(i), tile(j)] + outer(pair(2), i, j)).astype(BF16)
        ws[i * 2, :, tile(j)] = total[:PART]
        ws[i * 2 + 1, :, tile(j)] = total[PART:]

    bsum[...] += row_sums(2)
    for j in range(NZ):
        bsend[j] = bsum[:, j * DIM : (j + 1) * DIM]
    for dz in range(1, NZ):
        to = lax.rem(z + dz, NZ)
        remote(ws.at[to], wr.at[z], gr_send.at[0], gr_recv.at[0], {"sp_0": to}).start()
        remote(bsend.at[to], br.at[z], gr_send.at[1], gr_recv.at[1], {"sp_0": to}).start()
    pltpu.make_async_copy(ws.at[z], wr.at[z], gr_recv.at[0]).start()
    pltpu.make_async_copy(bsend.at[z], br.at[z], gr_recv.at[1]).start()

    gacc[...] = jnp.zeros_like(gacc)
    for a in range(2):
        for dx in (2, 1, 3, 0):
            xs = pair(dx)

            @pl.loop(0, NY)
            def _(t):
                if a == 0:
                    part = jnp.dot(WT[tile(t), :], Y[0, xs], preferred_element_type=F32).astype(BF16)
                    prod = part.astype(F32) * Y[1, xs, tile(t), :].astype(F32)
                    gacc[...] += jnp.sum(prod.reshape(ROWS // 8, 8, NC * DIM), axis=0)
                else:
                    rows = jnp.concatenate([W[t * 2], W[t * 2 + 1]], axis=0)
                    part = jnp.dot(rows, Y[1, xs], preferred_element_type=F32)
                    col = bcol[tile(t), :]
                    part = (part + jnp.concatenate([col, col], axis=1)).astype(BF16)
                R[a, xs, t, 0] = part[:, :DIM]
                R[a, xs, t, 1] = part[:, DIM:]

            for dy in range(1, NY):
                to = lax.rem(y + dy, NY)
                remote(R.at[a, xs, to], H.at[a, xs, y], yr_send, yr_recv.at[a, dx], {"sp_1": to}).start()
            pltpu.make_async_copy(R.at[a, xs, y], H.at[a, xs, y], yr_recv.at[a, dx]).start()
        if a == 0:
            line = jnp.sum(gacc[...], axis=0, keepdims=True)
            mine = pl.ds(pl.multiple_of((me * NY + y) * DIM, DIM), DIM)
            line = (line[:, :DIM] + line[:, DIM:]) / gain[0:1, mine]
            gsend[...] = jnp.broadcast_to(line, (8, DIM))
            for dz in range(1, NZ):
                remote(gsend, gz.at[z], gn_send.at[0], gn_recv.at[0], {"sp_0": lax.rem(z + dz, NZ)}).start()
            pltpu.make_async_copy(gsend, gz.at[z], gn_recv.at[0]).start()

    def home(a, dx):
        wait(H.at[a, pair(dx)], yr_recv.at[a, dx])
        xs = pair(dx)
        back_dx = (NX - dx) % NX
        for dc in range(NC):
            n = ORDER.index((back_dx, dc))
            cs = lax.rem(c + dc, NC)
            if n == 0:
                pltpu.make_async_copy(H.at[a, xs, :, cs], B.at[a, me], xr_recv.at[a, n]).start()
            else:
                remote(
                    H.at[a, xs, :, cs], B.at[a, me], xr_send, xr_recv.at[a, n],
                    {"dp_0": xs, "dp_1": cs},
                ).start()

    def arrived(a, n):
        xs, cs = from_xc(*ORDER[n])
        s = xs * NC + cs
        wait(B.at[a, s], xr_recv.at[a, n])
        return s

    for dx in (2, 1, 3, 0):
        home(0, dx)

    wait(gz, gn_recv.at[0])
    gxs[...] = jnp.sum(gz[...], axis=0)
    for n, d in enumerate(ORDER):
        xi, ci = at_xc(*d)
        if n == 0:
            pltpu.make_async_copy(gxs, gx.at[me], gn_recv.at[1]).start()
        else:
            remote(gxs, gx.at[me], gn_send.at[1], gn_recv.at[1], {"dp_0": xi, "dp_1": ci}).start()

    dot[...] = jnp.zeros_like(dot)
    for n in (0, 1, 2, 3, 4, 5, 6, 7):
        s = arrived(0, n)

        @pl.loop(0, ROWS // 32)
        def _(t):
            rows = pl.ds(pl.multiple_of(t * 32, 32), 32)
            total = dot[rows, :]
            for k in range(NY):
                at = pl.ds(pl.multiple_of((s * NY + k) * DIM, DIM), DIM)
                total += B[0, s, k, rows, :].astype(F32) * gain[0:1, at] * act[rows, at]
            dot[rows, :] = total

        if n == 3:
            home(1, 2)

    for dx in (1, 3, 0):
        home(1, dx)

    wait(gx, gn_recv.at[1])
    for i in range(NI):
        gys[i : i + 1, :] = gx[i, 0:1, :]
    for dy in range(1, NY):
        remote(gys, gy.at[y], gn_send.at[2], gn_recv.at[2], {"sp_1": lax.rem(y + dy, NY)}).start()
    pltpu.make_async_copy(gys, gy.at[y], gn_recv.at[2]).start()

    @pl.loop(0, ROWS // 16)
    def _(t):
        rows = pl.ds(pl.multiple_of(t * 16, 16), 16)
        scale = inv[rows, :]
        mean = jnp.sum(dot[rows, :], axis=1, keepdims=True) / WIDTH
        cube = scale * scale * scale * mean
        for g in range(NI * NY):
            at = slice(g * DIM, (g + 1) * DIM)
            scaled = B[0, g // NY, g % NY, rows, :].astype(F32) * gain[0:1, at]
            grad = (scale * scaled - cube * act[rows, at]) * sv[rows, at]
            val[rows, at] = grad.astype(BF16)

    pltpu.make_async_copy(val, valg_hbm, out_sem.at[0]).start()

    for n in (0, 1, 2, 3, 4, 5, 6, 7):
        s = arrived(1, n)

        @pl.loop(0, ROWS // 32)
        def _(t):
            rows = pl.ds(pl.multiple_of(t * 32, 32), 32)
            for k in range(NY):
                at = pl.ds(pl.multiple_of((s * NY + k) * DIM, DIM), DIM)
                mid = (cot[rows, at].astype(F32) * B[1, s, k, rows, :].astype(F32)).astype(BF16)
                up[rows, at] = (mid.astype(F32) * su[rows, at]).astype(BF16)

        pltpu.make_async_copy(up.at[:, cols(s)], upg_hbm.at[:, cols(s)], out_sem.at[1]).start()

    wait(wr, gr_recv.at[0])
    wait(br, gr_recv.at[1])

    @pl.loop(0, PART // 16)
    def _(t):
        rows = pl.ds(pl.multiple_of(t * 16, 16), 16)
        total = wr[0, rows, :].astype(F32)
        for k in range(1, NZ):
            total += wr[k, rows, :].astype(F32)
        wsum[rows, :] = total

    bsum[:, :DIM] = jnp.sum(br[...], axis=0)
    results = ((wsum, wout), (bsum.at[:, pl.ds(0, DIM)], bout))

    @pl.when(me != z)
    def _():
        for k, (src, dst) in enumerate(results):
            remote(src, dst, so_send.at[k], so_recv.at[k], swap_to).start()

    @pl.when(me == z)
    def _():
        for k, (src, dst) in enumerate(results):
            pltpu.make_async_copy(src, dst, so_recv.at[k]).start()

    wait(gy, gn_recv.at[2])
    tail = [pltpu.make_async_copy(gy, gg_hbm, out_sem.at[2])]
    tail[0].start()
    wait(wout, so_recv.at[0])
    wait(bout, so_recv.at[1])
    tail += [
        pltpu.make_async_copy(wout, wg_hbm, out_sem.at[3]),
        pltpu.make_async_copy(bout, bg_hbm, out_sem.at[4]),
    ]
    for copy in tail[1:]:
        copy.start()

    for a in range(2):
        wait(S.at[a, pl.ds(0, NI - 1)], xo_send)
        wait(H.at[a, pl.ds(0, 3)], xr_send)
        wait(H.at[a, 0, pl.ds(0, 2)], xr_send)
        wait(R.at[a, :, pl.ds(0, NY - 1)], yr_send)
        wait(X.at[a, :, pl.ds(0, NY - 1)], yo_send)
    wait(W.at[pl.ds(0, NZ - 1)], wz_send)
    wait(ws.at[pl.ds(0, NZ - 1)], gr_send.at[0])
    wait(bsend.at[pl.ds(0, NZ - 1)], gr_send.at[1])
    wait(gz.at[pl.ds(0, NZ - 1)], gn_send.at[0])
    wait(gx.at[pl.ds(0, NI - 1)], gn_send.at[1])
    wait(gy.at[pl.ds(0, NY - 1)], gn_send.at[2])

    @pl.when(me != z)
    def _():
        for k, (src, dst) in enumerate(moves):
            wait(src, sw_send.at[k])
        for k, (src, dst) in enumerate(results):
            wait(src, so_send.at[k])

    wait(val, out_sem.at[0])
    wait(up, out_sem.at[1])
    for copy in tail:
        copy.wait()


def shards(cotangent, up_pre, value_pre, spatial_weight, spatial_bias, value_gain):
    vmem, dma = pltpu.VMEM, pltpu.SemaphoreType.DMA
    tok = (ROWS, WIDTH)
    out = pl.pallas_call(
        kernel,
        name="gating_backward",
        out_shape=(
            jax.ShapeDtypeStruct(tok, BF16),
            jax.ShapeDtypeStruct(tok, BF16),
            jax.ShapeDtypeStruct((PART, BLOCK), F32),
            jax.ShapeDtypeStruct((8, DIM), F32),
            jax.ShapeDtypeStruct((NY, NI, DIM), F32),
        ),
        in_specs=[pl.BlockSpec(memory_space=pl.ANY)] * 6,
        out_specs=[pl.BlockSpec(memory_space=pl.ANY)] * 5,
        scratch_shapes=[
            vmem(tok, BF16), vmem(tok, BF16), vmem(tok, BF16),
            vmem((PART, BLOCK), BF16), vmem((1, BLOCK), F32), vmem((1, WIDTH), F32),
            vmem((2, NI, NY, ROWS, DIM), BF16),
            vmem((2, NI, NY, ROWS, DIM), BF16),
            vmem((2, NX, BLOCK, NC * DIM), BF16),
            vmem((2, NX, NY, NC, ROWS, DIM), BF16),
            vmem((2, NX, NY, NC, ROWS, DIM), BF16),
            vmem((2, NI, NY, ROWS, DIM), BF16),
            vmem((PART, BLOCK), BF16), vmem((1, BLOCK), F32),
            vmem((NZ, PART, BLOCK), BF16), vmem((BLOCK, BLOCK), BF16), vmem((BLOCK, DIM), F32),
            vmem((BLOCK, BLOCK), F32), vmem((NZ, PART, BLOCK), BF16), vmem((NZ, PART, BLOCK), BF16),
            vmem((PART, BLOCK), F32), vmem((PART, BLOCK), F32),
            vmem((NZ, 8, DIM), F32), vmem((NZ, 8, DIM), F32), vmem((8, BLOCK), F32), vmem((8, DIM), F32),
            vmem((8, DIM), F32), vmem((NZ, 8, DIM), F32), vmem((8, DIM), F32), vmem((NI, 8, DIM), F32),
            vmem((NI, DIM), F32), vmem((NY, NI, DIM), F32),
            vmem(tok, F32), vmem(tok, F32), vmem(tok, F32),
            vmem((ROWS, DIM), F32), vmem((ROWS, DIM), F32), vmem((8, NC * DIM), F32),
            dma((6,)), dma((5,)),
            dma(()), dma((2, NI)), dma(()), dma((2, NX)),
            dma((2,)), dma((2,)), dma(()), dma(()),
            dma(()), dma((2, NX)), dma(()), dma((2, NI)),
            dma((2,)), dma((2,)), dma((2,)), dma((2,)),
            dma((3,)), dma((3,)),
        ],
        compiler_params=pltpu.CompilerParams(
            collective_id=0, has_side_effects=True, vmem_limit_bytes=67043328
        ),
    )(
        cotangent[0], up_pre[0], value_pre[0], spatial_weight[0], spatial_bias, value_gain[None]
    )
    up_grad, value_grad, weight_grad, bias_grad, gain_grad = out
    gain_grad = gain_grad.transpose(1, 0, 2).reshape(WIDTH)
    return up_grad[None], value_grad[None], weight_grad[None], bias_grad[:1], gain_grad


def solution(mesh):
    torus = Mesh(mesh.devices.reshape(NZ, NY, NX, NC), ("sp_0", "sp_1", "dp_0", "dp_1"))
    in_specs = (
        P(DP, SP, None),
        P(DP, SP, None),
        P(DP, SP, None),
        P(SP, DP, None),
        P(SP, None),
        P(),
    )
    out_specs = (P(DP, SP, None), P(DP, SP, None), P(SP, DP, None), P(SP, DP), P())
    return jax.shard_map(
        shards, mesh=torus, in_specs=in_specs, out_specs=out_specs, check_vma=False
    )
```

```python
import math

import jax
import jax.numpy as jnp
from jax import lax
from jax.experimental import pallas as pl
from jax.experimental.pallas import tpu as pltpu
from jax.sharding import Mesh
from jax.sharding import PartitionSpec as P

SP = ("sp_0", "sp_1")
DP = ("dp_0", "dp_1")

NZ, NY, NX, NC = 8, 4, 4, 2
NI = NX * NC
ROWS = 256
DIM = 128
WIDTH = NI * NY * DIM
CHUNK = NY * DIM
BLOCK = NY * ROWS
PART = BLOCK // NZ
F32, BF16 = jnp.float32, jnp.bfloat16

norm_floor = 0.5
root_half = 1.0 / math.sqrt(2.0)
inv_root_tau = 1.0 / math.sqrt(2.0 * math.pi)

ORDER = ((0, 0), (0, 1), (1, 0), (3, 0), (1, 1), (3, 1), (2, 0), (2, 1))
NT = (((1,), (1,)), ((), ()))


def phi(x):
    return 0.5 * (1.0 + lax.erf(x * root_half))


def slope(x):
    return phi(x) + x * jnp.exp(-0.5 * x * x) * inv_root_tau


def kernel(
    cot_hbm, up_hbm, val_hbm, w_hbm, bias_hbm, gain_hbm,
    upg_hbm, valg_hbm, wg_hbm, bg_hbm, gg_hbm,
    cot, up, val, w_own, b_own, gain,
    S, X, V, Y, R0, R1, H0, H1, B,
    w_in, b_in, W, WT, bcol,
    ws, wr, far3, far4, wsum, wmid, wout, wfin, bsend, br, bsum, bmid, bout,
    gsend, gz, gxs, gx, gys, gy, gall,
    act, su, sv, inv, dot, gacc,
    in_sem, out_sem,
    xo_send, xo_recv, yo_send, yo_recv, vy_send, vy_recv, vx_send, vx_recv,
    sw_send, sw_recv, wz_send, wz_recv,
    yr_send, yr_recv, xr_send, xr_recv, mx_send, mx_recv, my_send, my_recv,
    gr_send, gr_recv, bi_send, bi_recv, so_send, so_recv,
    gn_send, gn_recv,
):
    z, y, x, c = (lax.axis_index(a) for a in ("sp_0", "sp_1", "dp_0", "dp_1"))
    me = x * NC + c

    def remote(src, dst, send, recv, where):
        return pltpu.make_async_remote_copy(
            src_ref=src, dst_ref=dst, send_sem=send, recv_sem=recv,
            device_id=where, device_id_type=pl.DeviceIdType.MESH,
        )

    def at_xc(dx, dc):
        return lax.rem(x + dx, NX), lax.rem(c + dc, NC)

    def from_xc(dx, dc):
        return lax.rem(x + NX - dx, NX), lax.rem(c + NC - dc, NC)

    def wait(ref, sem):
        pltpu.make_async_copy(ref, ref, sem).wait()

    loads = [
        pltpu.make_async_copy(src, dst, in_sem.at[k])
        for k, (src, dst) in enumerate(
            ((up_hbm, up), (cot_hbm, cot), (w_hbm, w_own), (bias_hbm, b_own), (val_hbm, val), (gain_hbm, gain))
        )
    ]
    for load in loads:
        load.start()

    barrier = pltpu.get_barrier_semaphore()

    def greet(where):
        pl.semaphore_signal(barrier, inc=1, device_id=where, device_id_type=pl.DeviceIdType.MESH)

    for dx, dc in ORDER[1:]:
        xi, ci = at_xc(dx, dc)
        greet({"dp_0": xi, "dp_1": ci})
    for dy in range(1, NY):
        greet({"sp_1": lax.rem(y + dy, NY)})
    for dz in range(1, NZ):
        greet({"sp_0": lax.rem(z + dz, NZ)})
    swap_to = {"sp_0": lax.rem(z + me, NZ), "dp_0": z // NC, "dp_1": lax.rem(z, NC)}
    turn = lax.rem(z + NZ - me, NZ)
    stays = me + z == 0

    @pl.when(jnp.logical_not(stays))
    def _():
        greet({"sp_0": me, "dp_0": turn // NC, "dp_1": lax.rem(turn, NC)})

    def cols(i):
        return pl.ds(pl.multiple_of(i * CHUNK, CHUNK), CHUNK)

    def gate_chunk(i):
        @pl.loop(0, ROWS // 32)
        def _(t):
            rows = pl.ds(pl.multiple_of(t * 32, 32), 32)
            u = up[rows, cols(i)].astype(F32)
            u = (u * phi(u)).astype(BF16).astype(F32)
            g = (cot[rows, cols(i)].astype(F32) * u).astype(BF16)
            for k in range(NY):
                S[0, i, k, rows, :] = g[:, k * DIM : (k + 1) * DIM]

    def span(k, n):
        return pl.ds(pl.multiple_of(k * n, n), n)

    def forward(n):
        xs, cs = from_xc(*ORDER[n])
        s = xs * NC + cs
        src = S.at[0, s] if n == 0 else X.at[s]
        dst = Y.at[0, span(y, ROWS), span(s, DIM)]
        for dy in range(1, NY):
            to = lax.rem(y + dy, NY)
            remote(src.at[to], dst, yo_send, yo_recv, {"sp_1": to}).start()
        pltpu.make_async_copy(src.at[y], dst, yo_recv).start()

    def push(n):
        if n == 0:
            forward(0)
            return
        xi, ci = at_xc(*ORDER[n])
        remote(
            S.at[0, xi * NC + ci], X.at[me], xo_send, xo_recv.at[n], {"dp_0": xi, "dp_1": ci}
        ).start()

    def relay(n):
        xs, cs = from_xc(*ORDER[n])
        wait(X.at[xs * NC + cs], xo_recv.at[n])
        forward(n)

    loads[0].wait()
    loads[1].wait()
    for d in ORDER:
        xi, ci = at_xc(*d)
        gate_chunk(xi * NC + ci)

    peers = NI - 1 + NY - 1 + NZ - 1

    @pl.when(jnp.logical_not(stays))
    def _():
        pl.semaphore_wait(barrier, peers + 1)

    @pl.when(stays)
    def _():
        pl.semaphore_wait(barrier, peers)

    loads[2].wait()
    loads[3].wait()
    moves = ((w_own, w_in), (b_own, b_in))

    @pl.when(jnp.logical_not(stays))
    def _():
        for k, (src, dst) in enumerate(moves):
            remote(src, dst, sw_send.at[k], sw_recv.at[k], swap_to).start()

    @pl.when(stays)
    def _():
        for k, (src, dst) in enumerate(moves):
            pltpu.make_async_copy(src, dst, sw_recv.at[k]).start()

    for n in range(NI):
        push(n)
    loads[4].wait()
    loads[5].wait()

    @pl.loop(0, ROWS // 16)
    def _(t):
        rows = pl.ds(pl.multiple_of(t * 16, 16), 16)
        total = jnp.zeros((16, DIM), F32)
        for i in range(NI):
            v = val[rows, i * CHUNK : (i + 1) * CHUNK].astype(F32)
            v = v * phi(v)
            act[rows, i * CHUNK : (i + 1) * CHUNK] = v
            v = v * v
            for k in range(NY):
                total += v[:, k * DIM : (k + 1) * DIM]
        scale = lax.rsqrt(jnp.sum(total, axis=1, keepdims=True) / WIDTH + norm_floor)
        inv[rows, :] = jnp.broadcast_to(scale, (16, DIM))
        for i in range(NI):
            for k in range(NY):
                at = slice((i * NY + k) * DIM, (i * NY + k + 1) * DIM)
                S[1, i, k, rows, :] = (act[rows, at] * scale * gain[0:1, at]).astype(BF16)

    for dy in range(1, NY):
        to = lax.rem(y + dy, NY)
        remote(S.at[1, :, to], V.at[:, span(y, ROWS)], vy_send, vy_recv, {"sp_1": to}).start()
    pltpu.make_async_copy(S.at[1, :, y], V.at[:, span(y, ROWS)], vy_recv).start()

    def slopes(src, dst):
        @pl.loop(0, ROWS // 32 * NI)
        def _(t):
            rows = pl.ds(pl.multiple_of(t // NI * 32, 32), 32)
            at = cols(lax.rem(t, NI))
            dst[rows, at] = slope(src[rows, at].astype(F32))

    relay(1)
    slopes(up, su)

    def along(dz):
        return lax.rem(z + dz, NZ)

    def part_of(dz):
        return lax.rem(turn + dz, NZ)

    half = PART // 2
    low, high = pl.ds(0, half), pl.ds(half, half)
    wait(w_in, sw_recv.at[0])
    wait(b_in, sw_recv.at[1])
    for dz in (1, 7, 2, 6):
        remote(w_in, W.at[turn], wz_send, wz_recv.at[dz], {"sp_0": along(dz)}).start()
    pltpu.make_async_copy(w_in, W.at[turn], wz_recv.at[0]).start()
    for n in (2, 3):
        relay(n)

    for k in range(BLOCK // DIM):
        part = jnp.broadcast_to(b_in[0:1, k * DIM : (k + 1) * DIM], (DIM, DIM))
        bcol[k * DIM : (k + 1) * DIM, :] = jnp.transpose(part)

    slopes(val, sv)

    for n in (4, 5):
        relay(n)
    wait(V, vy_recv)
    for n, d in enumerate(ORDER):
        xi, ci = at_xc(*d)
        dst = Y.at[1, :, span(me, DIM)]
        if n == 0:
            pltpu.make_async_copy(V.at[me], dst, vx_recv).start()
        else:
            remote(V.at[xi * NC + ci], dst, vx_send, vx_recv, {"dp_0": xi, "dp_1": ci}).start()
    for n in (6, 7):
        relay(n)

    def pair(dx):
        return lax.rem(x + NX - dx, NX)

    def tile(t):
        return span(t, ROWS)

    for dz, on, full, part, rows in ((6, 1, 3, 4, low), (2, 7, 5, 8, high)):
        kept = part_of(dz)
        wait(W.at[kept], wz_recv.at[NZ - dz])
        remote(W.at[kept], W.at[kept], wz_send, wz_recv.at[full], {"sp_0": along(on)}).start()
        remote(
            W.at[kept, rows], W.at[kept, rows], wz_send, wz_recv.at[part], {"sp_0": along(NZ - dz)}
        ).start()

    for dz, sem in ((0, 0), (7, 1), (1, 7), (5, 3), (3, 5)):
        wait(W.at[part_of(dz)], wz_recv.at[sem])
    wait(W.at[part_of(4), low], wz_recv.at[4])
    wait(W.at[part_of(4), high], wz_recv.at[8])

    @pl.loop(0, NZ)
    def _(j):
        WT[:, pl.ds(pl.multiple_of(j * PART, PART), PART)] = jnp.transpose(W[j])

    def back(dx):
        xs = pair(dx)

        @pl.loop(0, NY)
        def _(t):
            part = jnp.dot(WT[tile(t), :], Y[0, :, span(xs, NC * DIM)], preferred_element_type=F32)
            part = part.astype(BF16)
            R0[xs, t, 0] = part[:, :DIM]
            R0[xs, t, 1] = part[:, DIM:]

        for dy in range(1, NY):
            to = lax.rem(y + dy, NY)
            remote(R0.at[xs, to], H0.at[xs, y], yr_send, yr_recv.at[dx], {"sp_1": to}).start()
        pltpu.make_async_copy(R0.at[xs, y], H0.at[xs, y], yr_recv.at[dx]).start()

    def home(dx):
        xs = pair(dx)
        wait(H0.at[xs], yr_recv.at[dx])
        for dc in range(NC):
            n = ORDER.index(((NX - dx) % NX, dc))
            cs = lax.rem(c + dc, NC)
            src, dst = H0.at[xs, :, cs], B.at[0, me]
            if n == 0:
                pltpu.make_async_copy(src, dst, xr_recv.at[n]).start()
            else:
                remote(src, dst, xr_send, xr_recv.at[n], {"dp_0": xs, "dp_1": cs}).start()

    def mixed(dx):
        xs = pair(dx)

        @pl.loop(0, NY)
        def _(t):
            rows = jnp.concatenate([W[t * 2], W[t * 2 + 1]], axis=0)
            part = jnp.dot(rows, Y[1, :, span(xs, NC * DIM)], preferred_element_type=F32)
            col = bcol[tile(t), :]
            part = (part + jnp.concatenate([col, col], axis=1)).astype(BF16)
            R1[xs * NC, t] = part[:, :DIM]
            R1[xs * NC + 1, t] = part[:, DIM:]

        for dc in range(NC):
            n = ORDER.index(((NX - dx) % NX, dc))
            cs = lax.rem(c + dc, NC)
            if n > 0:
                remote(
                    R1.at[xs * NC + cs], H1.at[me], mx_send, mx_recv.at[n], {"dp_0": xs, "dp_1": cs}
                ).start()

    def settle(n):
        xs, cs = from_xc(*ORDER[n])
        s = xs * NC + cs
        if n > 0:
            wait(H1.at[s], mx_recv.at[n])
        src = (R1 if n == 0 else H1).at[s]
        for dy in range(1, NY):
            to = lax.rem(y + dy, NY)
            remote(src.at[to], B.at[1, s, y], my_send, my_recv.at[n], {"sp_1": to}).start()
        pltpu.make_async_copy(src.at[y], B.at[1, s, y], my_recv.at[n]).start()

    def arrived(a, n):
        xs, cs = from_xc(*ORDER[n])
        s = xs * NC + cs
        wait(B.at[a, s], (my_recv if a else xr_recv).at[n])
        return s

    wait(Y.at[0], yo_recv)
    back(1)
    back(3)
    wait(Y.at[1], vx_recv)
    mixed(2)

    @pl.loop(0, NY * NY)
    def _(t):
        i, j = t // NY, lax.rem(t, NY)
        total = lax.dot_general(Y[0, tile(i), :], Y[1, tile(j), :], NT, preferred_element_type=F32)
        total = total.astype(BF16)
        ws[i * 2, :, tile(j)] = total[:PART]
        ws[i * 2 + 1, :, tile(j)] = total[PART:]

    ones = jnp.ones((8, NI * DIM), BF16)
    bsum[...] = lax.dot_general(ones, Y[0], NT, preferred_element_type=F32)
    for j in range(NZ):
        bsend[j] = bsum[:, j * DIM : (j + 1) * DIM]

    for dz in range(1, NZ):
        remote(bsend.at[part_of(dz)], br.at[z], bi_send, bi_recv, {"sp_0": along(dz)}).start()
    pltpu.make_async_copy(bsend.at[turn], br.at[z], bi_recv).start()
    far = (
        (ws.at[part_of(3)], far3.at[0], gr_recv.at[0], 1),
        (ws.at[part_of(5)], far3.at[1], gr_recv.at[1], 7),
        (ws.at[part_of(4), low], far4.at[0], gr_recv.at[2], 2),
        (ws.at[part_of(4), high], far4.at[1], gr_recv.at[3], 6),
    )
    for src, dst, sem, dz in far:
        remote(src, dst, gr_send, sem, {"sp_0": along(dz)}).start()

    mixed(1)
    back(2)
    mixed(3)
    back(0)
    mixed(0)

    gacc[...] = jnp.zeros_like(gacc)

    @pl.loop(0, NX * NY)
    def _(t):
        xs, k = t // NY, lax.rem(t, NY)
        total = gacc[...]
        for cs in range(NC):
            part = R0[xs, k, cs].astype(F32) * Y[1, tile(k), span(xs * NC + cs, DIM)].astype(F32)
            total += jnp.sum(part.reshape(ROWS // 8, 8, DIM), axis=0)
        gacc[...] = total

    mine = pl.ds(pl.multiple_of((me * NY + y) * DIM, DIM), DIM)
    line = jnp.sum(gacc[...], axis=0, keepdims=True) / gain[0:1, mine]
    gsend[...] = jnp.broadcast_to(line, (8, DIM))
    for dz in range(1, NZ):
        remote(gsend, gz.at[z], gn_send.at[0], gn_recv.at[0], {"sp_0": along(dz)}).start()
    pltpu.make_async_copy(gsend, gz.at[z], gn_recv.at[0]).start()

    home(1)
    settle(6)
    settle(7)
    home(3)

    for k, (dz, rows) in enumerate(((2, low), (6, high))):
        wait(far3.at[k], gr_recv.at[k])
        wait(far4.at[k], gr_recv.at[2 + k])
        to = part_of(dz)
        ws[to] = (ws[to].astype(F32) + far3[k].astype(F32)).astype(BF16)
        ws[to, rows] = (ws[to, rows].astype(F32) + far4[k].astype(F32)).astype(BF16)
        remote(ws.at[to], wr.at[2 + k], gr_send, gr_recv.at[6 + k], {"sp_0": along(dz)}).start()

    for k, dz in enumerate((1, 7)):
        remote(ws.at[part_of(dz)], wr.at[k], gr_send, gr_recv.at[4 + k], {"sp_0": along(dz)}).start()

    wait(gz, gn_recv.at[0])
    gxs[...] = jnp.sum(gz[...], axis=0)
    for n, d in enumerate(ORDER):
        xi, ci = at_xc(*d)
        if n == 0:
            pltpu.make_async_copy(gxs, gx.at[me], gn_recv.at[1]).start()
        else:
            remote(gxs, gx.at[me], gn_send.at[1], gn_recv.at[1], {"dp_0": xi, "dp_1": ci}).start()

    home(2)
    for dc in range(NC):
        settle(ORDER.index((3, dc)))
    for dc in range(NC):
        settle(ORDER.index((1, dc)))
    home(0)
    settle(1)
    settle(0)

    def finish_gain():
        wait(gx, gn_recv.at[1])
        for i in range(NI):
            gys[i : i + 1, :] = gx[i, 0:1, :]
        for dy in range(1, NY):
            remote(gys, gy.at[y], gn_send.at[2], gn_recv.at[2], {"sp_1": lax.rem(y + dy, NY)}).start()
        pltpu.make_async_copy(gys, gy.at[y], gn_recv.at[2]).start()

    dot[...] = jnp.zeros_like(dot)

    def row_sums(n):
        s = arrived(0, n)

        @pl.loop(0, ROWS // 32)
        def _(t):
            rows = pl.ds(pl.multiple_of(t * 32, 32), 32)
            total = dot[rows, :]
            for k in range(NY):
                at = pl.ds(pl.multiple_of((s * NY + k) * DIM, DIM), DIM)
                total += B[0, s, k, rows, :].astype(F32) * gain[0:1, at] * act[rows, at]
            dot[rows, :] = total

    for n in (2, 3, 4, 5):
        row_sums(n)

    for k in range(4):
        wait(wr.at[k], gr_recv.at[4 + k])
    wait(br, bi_recv)

    @pl.loop(0, PART // 16)
    def _(t):
        rows = pl.ds(pl.multiple_of(t * 16, 16), 16)
        total = ws[turn, rows, :].astype(F32)
        for k in range(4):
            total += wr[k, rows, :].astype(F32)
        wsum[rows, :] = total.astype(BF16)

    bsum[:, :DIM] = jnp.sum(br[...], axis=0)
    first = ((wsum, wmid), (bsum.at[:, pl.ds(0, DIM)], bmid))
    second = ((wmid, wout), (bmid, bout))

    @pl.when(turn != me)
    def _():
        for k, (src, dst) in enumerate(first):
            remote(
                src, dst, so_send.at[k], so_recv.at[k], {"dp_0": turn // NC, "dp_1": lax.rem(turn, NC)}
            ).start()

    @pl.when(turn == me)
    def _():
        for k, (src, dst) in enumerate(first):
            pltpu.make_async_copy(src, dst, so_recv.at[k]).start()

    for n in (6, 7, 1, 0):
        row_sums(n)

    wait(wmid, so_recv.at[0])
    wait(bmid, so_recv.at[1])

    @pl.when(me != 0)
    def _():
        for k, (src, dst) in enumerate(second):
            remote(src, dst, so_send.at[2 + k], so_recv.at[2 + k], {"sp_0": turn}).start()

    @pl.when(me == 0)
    def _():
        for k, (src, dst) in enumerate(second):
            pltpu.make_async_copy(src, dst, so_recv.at[2 + k]).start()

    @pl.loop(0, ROWS // 16)
    def _(t):
        rows = pl.ds(pl.multiple_of(t * 16, 16), 16)
        scale = inv[rows, :]
        mean = jnp.sum(dot[rows, :], axis=1, keepdims=True) / WIDTH
        cube = scale * scale * scale * mean
        for g in range(NI * NY):
            at = slice(g * DIM, (g + 1) * DIM)
            scaled = B[0, g // NY, g % NY, rows, :].astype(F32) * gain[0:1, at]
            grad = (scale * scaled - cube * act[rows, at]) * sv[rows, at]
            val[rows, at] = grad.astype(BF16)

    pltpu.make_async_copy(val, valg_hbm, out_sem.at[0]).start()

    def finish(n):
        s = arrived(1, n)

        @pl.loop(0, ROWS // 32)
        def _(t):
            rows = pl.ds(pl.multiple_of(t * 32, 32), 32)
            for k in range(NY):
                at = pl.ds(pl.multiple_of((s * NY + k) * DIM, DIM), DIM)
                mid = (cot[rows, at].astype(F32) * B[1, s, k, rows, :].astype(F32)).astype(BF16)
                up[rows, at] = (mid.astype(F32) * su[rows, at]).astype(BF16)

        pltpu.make_async_copy(up.at[:, cols(s)], upg_hbm.at[:, cols(s)], out_sem.at[1]).start()

    for n in (2, 3):
        finish(n)
    finish_gain()
    for n in (4, 5, 6, 7, 1, 0):
        finish(n)

    wait(gy, gn_recv.at[2])
    for i in range(NI):
        for k in range(NY):
            gall[i * NY + k : i * NY + k + 1, :] = gy[k, i : i + 1, :]
    tail = [pltpu.make_async_copy(gall, gg_hbm, out_sem.at[2])]
    tail[0].start()
    wait(wout, so_recv.at[2])
    wait(bout, so_recv.at[3])
    wfin[...] = wout[...].astype(F32)
    tail += [
        pltpu.make_async_copy(wfin, wg_hbm, out_sem.at[3]),
        pltpu.make_async_copy(bout, bg_hbm, out_sem.at[4]),
    ]
    for copy in tail[1:]:
        copy.start()

    wait(X.at[pl.ds(0, NI - 1)], xo_send)
    wait(X.at[:, pl.ds(0, NY - 1)], yo_send)
    wait(S.at[1, :, pl.ds(0, NY - 1)], vy_send)
    wait(V.at[pl.ds(0, NI - 1)], vx_send)
    wait(R0.at[:, pl.ds(0, NY - 1)], yr_send)
    wait(B.at[0, pl.ds(0, NI - 1)], xr_send)
    wait(H1.at[pl.ds(0, NI - 1)], mx_send)
    wait(B.at[1, :, pl.ds(0, NY - 1)], my_send)
    wait(W.at[pl.ds(0, NZ - 1)], wz_send)
    wait(ws.at[pl.ds(0, NZ - 1)], gr_send)
    wait(bsend.at[pl.ds(0, NZ - 1)], bi_send)
    wait(gz.at[pl.ds(0, NZ - 1)], gn_send.at[0])
    wait(gx.at[pl.ds(0, NI - 1)], gn_send.at[1])
    wait(gy.at[pl.ds(0, NY - 1)], gn_send.at[2])

    @pl.when(jnp.logical_not(stays))
    def _():
        for k, (src, dst) in enumerate(moves):
            wait(src, sw_send.at[k])

    @pl.when(turn != me)
    def _():
        for k, (src, dst) in enumerate(first):
            wait(src, so_send.at[k])

    @pl.when(me != 0)
    def _():
        for k, (src, dst) in enumerate(second):
            wait(src, so_send.at[2 + k])

    wait(val, out_sem.at[0])
    wait(up, out_sem.at[1])
    for copy in tail:
        copy.wait()


def shards(cotangent, up_pre, value_pre, spatial_weight, spatial_bias, value_gain):
    vmem, dma = pltpu.VMEM, pltpu.SemaphoreType.DMA
    tok = (ROWS, WIDTH)
    out = pl.pallas_call(
        kernel,
        name="gating_backward",
        out_shape=(
            jax.ShapeDtypeStruct(tok, BF16),
            jax.ShapeDtypeStruct(tok, BF16),
            jax.ShapeDtypeStruct((PART, BLOCK), F32),
            jax.ShapeDtypeStruct((8, DIM), F32),
            jax.ShapeDtypeStruct((NY * NI, DIM), F32),
        ),
        in_specs=[pl.BlockSpec(memory_space=pl.ANY)] * 6,
        out_specs=[pl.BlockSpec(memory_space=pl.ANY)] * 5,
        scratch_shapes=[
            vmem(tok, BF16), vmem(tok, BF16), vmem(tok, BF16),
            vmem((PART, BLOCK), BF16), vmem((1, BLOCK), F32), vmem((1, WIDTH), F32),
            vmem((2, NI, NY, ROWS, DIM), BF16),
            vmem((NI, NY, ROWS, DIM), BF16),
            vmem((NI, BLOCK, DIM), BF16),
            vmem((2, BLOCK, NI * DIM), BF16),
            vmem((NX, NY, NC, ROWS, DIM), BF16), vmem((NI, NY, ROWS, DIM), BF16),
            vmem((NX, NY, NC, ROWS, DIM), BF16), vmem((NI, NY, ROWS, DIM), BF16),
            vmem((2, NI, NY, ROWS, DIM), BF16),
            vmem((PART, BLOCK), BF16), vmem((1, BLOCK), F32),
            vmem((NZ, PART, BLOCK), BF16), vmem((BLOCK, BLOCK), BF16), vmem((BLOCK, DIM), F32),
            vmem((NZ, PART, BLOCK), BF16), vmem((4, PART, BLOCK), BF16),
            vmem((2, PART, BLOCK), BF16), vmem((2, PART // 2, BLOCK), BF16),
            vmem((PART, BLOCK), BF16), vmem((PART, BLOCK), BF16), vmem((PART, BLOCK), BF16),
            vmem((PART, BLOCK), F32),
            vmem((NZ, 8, DIM), F32), vmem((NZ, 8, DIM), F32), vmem((8, BLOCK), F32),
            vmem((8, DIM), F32), vmem((8, DIM), F32),
            vmem((8, DIM), F32), vmem((NZ, 8, DIM), F32), vmem((8, DIM), F32), vmem((NI, 8, DIM), F32),
            vmem((NI, DIM), F32), vmem((NY, NI, DIM), F32), vmem((NY * NI, DIM), F32),
            vmem(tok, F32), vmem(tok, F32), vmem(tok, F32),
            vmem((ROWS, DIM), F32), vmem((ROWS, DIM), F32), vmem((8, DIM), F32),
            dma((6,)), dma((5,)),
            dma(()), dma((NI,)), dma(()), dma(()), dma(()), dma(()), dma(()), dma(()),
            dma((2,)), dma((2,)), dma(()), dma((9,)),
            dma(()), dma((NX,)), dma(()), dma((NI,)), dma(()), dma((NI,)), dma(()), dma((NI,)),
            dma(()), dma((8,)), dma(()), dma(()), dma((4,)), dma((4,)),
            dma((3,)), dma((3,)),
        ],
        compiler_params=pltpu.CompilerParams(
            collective_id=0, has_side_effects=True, vmem_limit_bytes=67043328
        ),
    )(
        cotangent[0], up_pre[0], value_pre[0], spatial_weight[0], spatial_bias, value_gain[None]
    )
    up_grad, value_grad, weight_grad, bias_grad, gain_grad = out
    return up_grad[None], value_grad[None], weight_grad[None], bias_grad[:1], gain_grad.reshape(WIDTH)


def solution(mesh):
    torus = Mesh(mesh.devices.reshape(NZ, NY, NX, NC), ("sp_0", "sp_1", "dp_0", "dp_1"))
    in_specs = (
        P(DP, SP, None),
        P(DP, SP, None),
        P(DP, SP, None),
        P(SP, DP, None),
        P(SP, None),
        P(),
    )
    out_specs = (P(DP, SP, None), P(DP, SP, None), P(SP, DP, None), P(SP, DP), P())
    return jax.shard_map(
        shards, mesh=torus, in_specs=in_specs, out_specs=out_specs, check_vma=False
    )
```

```python
import math

import jax
import jax.numpy as jnp
from jax import lax
from jax.experimental import pallas as pl
from jax.experimental.pallas import tpu as pltpu
from jax.sharding import Mesh
from jax.sharding import PartitionSpec as P

SP = ("sp_0", "sp_1")
DP = ("dp_0", "dp_1")

NZ, NY, NX, NC = 8, 4, 4, 2
NI = NX * NC
ROWS = 256
DIM = 128
WIDTH = NI * NY * DIM
CHUNK = NY * DIM
BLOCK = NY * ROWS
PART = BLOCK // NZ
F32, BF16 = jnp.float32, jnp.bfloat16

norm_floor = 0.5
root_half = 1.0 / math.sqrt(2.0)
inv_root_tau = 1.0 / math.sqrt(2.0 * math.pi)

ORDER = ((0, 0), (0, 1), (1, 0), (3, 0), (1, 1), (3, 1), (2, 0), (2, 1))
NT = (((1,), (1,)), ((), ()))


def phi(x):
    return 0.5 * (1.0 + lax.erf(x * root_half))


def slope(x):
    return phi(x) + x * jnp.exp(-0.5 * x * x) * inv_root_tau


def kernel(
    cot_hbm, up_hbm, val_hbm, w_hbm, bias_hbm, gain_hbm,
    upg, valg, wout, bout, gall,
    cot, up, val, w_own, b_own, gain,
    S, X, V, Y, R0, R1, H0, H1, B,
    w_in, b_in, W, WT, bcol,
    ws, wr, far3, far4, wsum, wmid, bsend, br, bsum, bmid,
    gsend, gz, gxs, gx, gys, gy,
    act, su, sv, inv, dot, gacc,
    in_sem,
    xo_send, xo_recv, yo_send, yo_recv, vy_send, vy_recv, vx_send, vx_recv,
    sw_send, sw_recv, wz_send, wz_recv,
    yr_send, yr_recv, xr_send, xr_recv, mx_send, mx_recv, my_send, my_recv,
    gr_send, gr_recv, bi_send, bi_recv, so_send, so_recv,
    gn_send, gn_recv,
):
    z, y, x, c = (lax.axis_index(a) for a in ("sp_0", "sp_1", "dp_0", "dp_1"))
    me = x * NC + c

    def remote(src, dst, send, recv, where):
        return pltpu.make_async_remote_copy(
            src_ref=src, dst_ref=dst, send_sem=send, recv_sem=recv,
            device_id=where, device_id_type=pl.DeviceIdType.MESH,
        )

    def at_xc(dx, dc):
        return lax.rem(x + dx, NX), lax.rem(c + dc, NC)

    def from_xc(dx, dc):
        return lax.rem(x + NX - dx, NX), lax.rem(c + NC - dc, NC)

    def wait(ref, sem):
        pltpu.make_async_copy(ref, ref, sem).wait()

    loads = [
        pltpu.make_async_copy(src, dst, in_sem.at[k])
        for k, (src, dst) in enumerate(
            ((up_hbm, up), (cot_hbm, cot), (w_hbm, w_own), (bias_hbm, b_own), (val_hbm, val), (gain_hbm, gain))
        )
    ]
    for k in (4, 5, 2, 3, 0, 1):
        loads[k].start()

    barrier = pltpu.get_barrier_semaphore()

    def greet(where):
        pl.semaphore_signal(barrier, inc=1, device_id=where, device_id_type=pl.DeviceIdType.MESH)

    for dx, dc in ORDER[1:]:
        xi, ci = at_xc(dx, dc)
        greet({"dp_0": xi, "dp_1": ci})
    for dy in range(1, NY):
        greet({"sp_1": lax.rem(y + dy, NY)})
    for dz in range(1, NZ):
        greet({"sp_0": lax.rem(z + dz, NZ)})
    shift = x + c * NX
    swap_to = {"sp_0": lax.rem(z + shift, NZ), "dp_0": z // NC, "dp_1": lax.rem(z, NC)}
    turn = lax.rem(z + NZ - me, NZ)

    def part_of(dz):
        t = lax.rem(turn + dz, NZ)
        return lax.rem(t, NX) * NC + t // NX

    mine = part_of(0)
    swap_from = {"sp_0": me, "dp_0": mine // NC, "dp_1": lax.rem(mine, NC)}
    stays = me + z == 0

    @pl.when(jnp.logical_not(stays))
    def _():
        greet(swap_from)
        greet(swap_to)

    def cols(i):
        return pl.ds(pl.multiple_of(i * CHUNK, CHUNK), CHUNK)

    def gate_chunk(i):
        @pl.loop(0, ROWS // 32)
        def _(t):
            rows = pl.ds(pl.multiple_of(t * 32, 32), 32)
            u = up[rows, cols(i)].astype(F32)
            u = (u * phi(u)).astype(BF16).astype(F32)
            g = (cot[rows, cols(i)].astype(F32) * u).astype(BF16)
            for k in range(NY):
                S[0, i, k, rows, :] = g[:, k * DIM : (k + 1) * DIM]

    def span(k, n):
        return pl.ds(pl.multiple_of(k * n, n), n)

    def forward(n):
        xs, cs = from_xc(*ORDER[n])
        s = xs * NC + cs
        src = S.at[0, s] if n == 0 else X.at[s]
        dst = Y.at[0, span(y, ROWS), span(s, DIM)]
        for dy in range(1, NY):
            to = lax.rem(y + dy, NY)
            remote(src.at[to], dst, yo_send, yo_recv, {"sp_1": to}).start()
        pltpu.make_async_copy(src.at[y], dst, yo_recv).start()

    def push(n):
        xi, ci = at_xc(*ORDER[n])
        remote(
            S.at[0, xi * NC + ci], X.at[me], xo_send, xo_recv.at[n], {"dp_0": xi, "dp_1": ci}
        ).start()

    def relay(n):
        xs, cs = from_xc(*ORDER[n])
        wait(X.at[xs * NC + cs], xo_recv.at[n])
        forward(n)

    loads[4].wait()
    loads[5].wait()

    @pl.loop(0, ROWS // 16)
    def _(t):
        rows = pl.ds(pl.multiple_of(t * 16, 16), 16)
        total = jnp.zeros((16, DIM), F32)
        for i in range(NI):
            v = val[rows, i * CHUNK : (i + 1) * CHUNK].astype(F32)
            v = v * phi(v)
            act[rows, i * CHUNK : (i + 1) * CHUNK] = v
            v = v * v
            for k in range(NY):
                total += v[:, k * DIM : (k + 1) * DIM]
        scale = lax.rsqrt(jnp.sum(total, axis=1, keepdims=True) / WIDTH + norm_floor)
        inv[rows, :] = jnp.broadcast_to(scale, (16, DIM))
        for i in range(NI):
            for k in range(NY):
                at = slice((i * NY + k) * DIM, (i * NY + k + 1) * DIM)
                S[1, i, k, rows, :] = (act[rows, at] * scale * gain[0:1, at]).astype(BF16)

    peers = NI - 1 + NY - 1 + NZ - 1

    @pl.when(jnp.logical_not(stays))
    def _():
        pl.semaphore_wait(barrier, peers + 2)

    @pl.when(stays)
    def _():
        pl.semaphore_wait(barrier, peers)

    loads[2].wait()
    loads[3].wait()
    moves = ((w_own, w_in), (b_own, b_in))

    def quarters(src, dst, send, recv, where):
        for k in range(4):
            rows = pl.ds(k * (PART // 4), PART // 4)
            remote(src.at[rows], dst.at[rows], send, recv, where).start()

    @pl.when(jnp.logical_not(stays))
    def _():
        quarters(w_own, w_in, sw_send.at[0], sw_recv.at[0], swap_to)
        remote(b_own, b_in, sw_send.at[1], sw_recv.at[1], swap_to).start()

    @pl.when(stays)
    def _():
        for k, (src, dst) in enumerate(moves):
            pltpu.make_async_copy(src, dst, sw_recv.at[k]).start()

    for dy in range(1, NY):
        to = lax.rem(y + dy, NY)
        remote(S.at[1, :, to], V.at[:, span(y, ROWS)], vy_send, vy_recv, {"sp_1": to}).start()
    pltpu.make_async_copy(S.at[1, :, y], V.at[:, span(y, ROWS)], vy_recv).start()

    loads[0].wait()
    loads[1].wait()
    for n, d in enumerate(ORDER):
        xi, ci = at_xc(*d)
        gate_chunk(xi * NC + ci)
        if n > 1:
            push(n - 1)
    push(NI - 1)

    def slopes(src, dst):
        @pl.loop(0, ROWS // 32 * NI)
        def _(t):
            rows = pl.ds(pl.multiple_of(t // NI * 32, 32), 32)
            at = cols(lax.rem(t, NI))
            dst[rows, at] = slope(src[rows, at].astype(F32))

    slopes(up, su)

    def along(dz):
        return lax.rem(z + dz, NZ)

    half = PART // 2
    low, high = pl.ds(0, half), pl.ds(half, half)
    wait(w_in, sw_recv.at[0])
    wait(b_in, sw_recv.at[1])
    for dz in (1, 7, 2, 6):
        remote(w_in, W.at[mine], wz_send, wz_recv.at[dz], {"sp_0": along(dz)}).start()
    pltpu.make_async_copy(w_in, W.at[mine], wz_recv.at[0]).start()

    for k in range(BLOCK // DIM):
        part = jnp.broadcast_to(b_in[0:1, k * DIM : (k + 1) * DIM], (DIM, DIM))
        bcol[k * DIM : (k + 1) * DIM, :] = jnp.transpose(part)

    slopes(val, sv)

    wait(V, vy_recv)
    for n, d in enumerate(ORDER):
        xi, ci = at_xc(*d)
        dst = Y.at[1, :, span(me, DIM)]
        if n == 0:
            pltpu.make_async_copy(V.at[me], dst, vx_recv.at[d[0]]).start()
        else:
            remote(V.at[xi * NC + ci], dst, vx_send, vx_recv.at[d[0]], {"dp_0": xi, "dp_1": ci}).start()
    for n in (2, 3, 4, 5):
        relay(n)
    forward(0)
    for n in (1, 6, 7):
        relay(n)

    def pair(dx):
        return lax.rem(x + NX - dx, NX)

    def tile(t):
        return span(t, ROWS)

    for dz, on, full, part, rows in ((6, 1, 3, 4, low), (2, 7, 5, 8, high)):
        kept = part_of(dz)
        wait(W.at[kept], wz_recv.at[NZ - dz])
        remote(W.at[kept], W.at[kept], wz_send, wz_recv.at[full], {"sp_0": along(on)}).start()
        remote(
            W.at[kept, rows], W.at[kept, rows], wz_send, wz_recv.at[part], {"sp_0": along(NZ - dz)}
        ).start()

    for dz, sem in ((0, 0), (7, 1), (1, 7), (5, 3), (3, 5)):
        wait(W.at[part_of(dz)], wz_recv.at[sem])
    wait(W.at[part_of(4), low], wz_recv.at[4])
    wait(W.at[part_of(4), high], wz_recv.at[8])

    def back(dx):
        xs = pair(dx)

        @pl.loop(0, NY)
        def _(t):
            part = jnp.dot(WT[tile(t), :], Y[0, :, span(xs, NC * DIM)], preferred_element_type=F32)
            part = part.astype(BF16)
            R0[xs, t, 0] = part[:, :DIM]
            R0[xs, t, 1] = part[:, DIM:]

        for dy in range(1, NY):
            to = lax.rem(y + dy, NY)
            remote(R0.at[xs, to], H0.at[xs, y], yr_send, yr_recv.at[dx], {"sp_1": to}).start()
        pltpu.make_async_copy(R0.at[xs, y], H0.at[xs, y], yr_recv.at[dx]).start()

    def home(dx):
        xs = pair(dx)
        wait(H0.at[xs], yr_recv.at[dx])
        for dc in range(NC):
            n = ORDER.index(((NX - dx) % NX, dc))
            cs = lax.rem(c + dc, NC)
            src, dst = H0.at[xs, :, cs], B.at[0, me]
            if n == 0:
                pltpu.make_async_copy(src, dst, xr_recv.at[n]).start()
            else:
                remote(src, dst, xr_send, xr_recv.at[n], {"dp_0": xs, "dp_1": cs}).start()

    def mixed(dx):
        xs = pair(dx)

        @pl.loop(0, NY)
        def _(t):
            rows = jnp.concatenate([W[t * 2], W[t * 2 + 1]], axis=0)
            part = jnp.dot(rows, Y[1, :, span(xs, NC * DIM)], preferred_element_type=F32)
            col = bcol[tile(t), :]
            part = (part + jnp.concatenate([col, col], axis=1)).astype(BF16)
            R1[xs * NC, t] = part[:, :DIM]
            R1[xs * NC + 1, t] = part[:, DIM:]

        for dc in range(NC):
            n = ORDER.index(((NX - dx) % NX, dc))
            cs = lax.rem(c + dc, NC)
            if n > 0:
                remote(
                    R1.at[xs * NC + cs], H1.at[me], mx_send, mx_recv.at[n], {"dp_0": xs, "dp_1": cs}
                ).start()

    def settle(n):
        xs, cs = from_xc(*ORDER[n])
        s = xs * NC + cs
        if n > 0:
            wait(H1.at[s], mx_recv.at[n])
        src = (R1 if n == 0 else H1).at[s]
        for dy in range(1, NY):
            to = lax.rem(y + dy, NY)
            remote(src.at[to], B.at[1, s, y], my_send, my_recv.at[n], {"sp_1": to}).start()
        pltpu.make_async_copy(src.at[y], B.at[1, s, y], my_recv.at[n]).start()

    def arrived(a, n):
        xs, cs = from_xc(*ORDER[n])
        s = xs * NC + cs
        wait(B.at[a, s], (my_recv if a else xr_recv).at[n])
        return s

    def value_pair(dx):
        wait(Y.at[1, :, span(pair(dx), NC * DIM)], vx_recv.at[dx])

    def outer(p, q):
        p, q = part_of(p), part_of(q)

        @pl.loop(0, NY)
        def _(j):
            rows = jnp.concatenate([Y[0, span(p, PART), :], Y[0, span(q, PART), :]], axis=0)
            total = lax.dot_general(rows, Y[1, tile(j), :], NT, preferred_element_type=F32).astype(BF16)
            ws[p, :, tile(j)] = total[:PART]
            ws[q, :, tile(j)] = total[PART:]

    value_pair(1)
    mixed(1)
    value_pair(3)
    mixed(3)

    @pl.loop(0, NZ)
    def _(j):
        WT[:, pl.ds(pl.multiple_of(j * PART, PART), PART)] = jnp.transpose(W[j])

    wait(Y.at[0], yo_recv)
    back(1)
    value_pair(2)
    value_pair(0)

    outer(3, 5)
    remote(ws.at[part_of(3)], far3.at[0], gr_send, gr_recv.at[0], {"sp_0": along(1)}).start()
    remote(ws.at[part_of(5)], far3.at[1], gr_send, gr_recv.at[1], {"sp_0": along(7)}).start()
    outer(4, 2)
    remote(ws.at[part_of(4), low], far4.at[0], gr_send, gr_recv.at[2], {"sp_0": along(2)}).start()
    remote(ws.at[part_of(4), high], far4.at[1], gr_send, gr_recv.at[3], {"sp_0": along(6)}).start()
    back(3)
    mixed(2)
    back(2)
    outer(6, 1)
    outer(7, 0)

    ones = jnp.ones((8, NI * DIM), BF16)
    bsum[...] = lax.dot_general(ones, Y[0], NT, preferred_element_type=F32)
    for j in range(NZ):
        bsend[j] = bsum[:, j * DIM : (j + 1) * DIM]
    back(0)
    mixed(0)
    for dz in range(1, NZ):
        remote(bsend.at[part_of(dz)], br.at[z], bi_send, bi_recv, {"sp_0": along(dz)}).start()
    pltpu.make_async_copy(bsend.at[mine], br.at[z], bi_recv).start()

    gacc[...] = jnp.zeros_like(gacc)

    @pl.loop(0, NX * NY)
    def _(t):
        xs, k = t // NY, lax.rem(t, NY)
        total = gacc[...]
        for cs in range(NC):
            part = R0[xs, k, cs].astype(F32) * Y[1, tile(k), span(xs * NC + cs, DIM)].astype(F32)
            total += jnp.sum(part.reshape(ROWS // 8, 8, DIM), axis=0)
        gacc[...] = total

    line = jnp.sum(gacc[...], axis=0, keepdims=True) / gain[0:1, span(me * NY + y, DIM)]
    gsend[...] = jnp.broadcast_to(line, (8, DIM))
    for dz in range(1, NZ):
        remote(gsend, gz.at[z], gn_send.at[0], gn_recv.at[0], {"sp_0": along(dz)}).start()
    pltpu.make_async_copy(gsend, gz.at[z], gn_recv.at[0]).start()

    home(1)
    home(3)

    for k, (dz, rows) in enumerate(((2, low), (6, high))):
        wait(far3.at[k], gr_recv.at[k])
        wait(far4.at[k], gr_recv.at[2 + k])
        to = part_of(dz)
        ws[to] = (ws[to].astype(F32) + far3[k].astype(F32)).astype(BF16)
        ws[to, rows] = (ws[to, rows].astype(F32) + far4[k].astype(F32)).astype(BF16)
        remote(ws.at[to], wr.at[2 + k], gr_send, gr_recv.at[6 + k], {"sp_0": along(dz)}).start()

    for k, dz in enumerate((1, 7)):
        remote(ws.at[part_of(dz)], wr.at[k], gr_send, gr_recv.at[4 + k], {"sp_0": along(dz)}).start()

    for dx in (3, 1):
        for dc in range(NC):
            settle(ORDER.index((dx, dc)))
    home(2)

    settle(1)
    settle(0)
    home(0)
    settle(6)
    settle(7)

    wait(gz, gn_recv.at[0])
    gxs[...] = jnp.sum(gz[...], axis=0)
    for n, d in enumerate(ORDER):
        xi, ci = at_xc(*d)
        if n == 0:
            pltpu.make_async_copy(gxs, gx.at[me], gn_recv.at[1]).start()
        else:
            remote(gxs, gx.at[me], gn_send.at[1], gn_recv.at[1], {"dp_0": xi, "dp_1": ci}).start()

    def finish_gain():
        wait(gx, gn_recv.at[1])
        for i in range(NI):
            gys[i : i + 1, :] = gx[i, 0:1, :]
        for dy in range(1, NY):
            remote(gys, gy.at[y], gn_send.at[2], gn_recv.at[2], {"sp_1": lax.rem(y + dy, NY)}).start()
        pltpu.make_async_copy(gys, gy.at[y], gn_recv.at[2]).start()

    def finish(n):
        s = arrived(1, n)

        @pl.loop(0, ROWS // 32)
        def _(t):
            rows = pl.ds(pl.multiple_of(t * 32, 32), 32)
            for k in range(NY):
                at = pl.ds(pl.multiple_of((s * NY + k) * DIM, DIM), DIM)
                mid = (cot[rows, at].astype(F32) * B[1, s, k, rows, :].astype(F32)).astype(BF16)
                upg[rows, at] = (mid.astype(F32) * su[rows, at]).astype(BF16)

    dot[...] = jnp.zeros_like(dot)

    def row_sums(n):
        s = arrived(0, n)

        @pl.loop(0, ROWS // 32)
        def _(t):
            rows = pl.ds(pl.multiple_of(t * 32, 32), 32)
            total = dot[rows, :]
            for k in range(NY):
                at = pl.ds(pl.multiple_of((s * NY + k) * DIM, DIM), DIM)
                total += B[0, s, k, rows, :].astype(F32) * gain[0:1, at] * act[rows, at]
            dot[rows, :] = total

    for n in (2, 3):
        row_sums(n)

    for k in range(4):
        wait(wr.at[k], gr_recv.at[4 + k])
    wait(br, bi_recv)

    @pl.loop(0, PART // 16)
    def _(t):
        rows = pl.ds(pl.multiple_of(t * 16, 16), 16)
        total = ws[mine, rows, :].astype(F32)
        for k in range(4):
            total += wr[k, rows, :].astype(F32)
        wsum[rows, :] = total.astype(BF16)

    bsum[:, :DIM] = jnp.sum(br[...], axis=0)
    first = ((wsum.at[low], wmid), (bsum.at[:, pl.ds(0, DIM)], bmid))
    second = ((wmid, wout.at[low]), (bmid, bout))

    @pl.when(jnp.logical_not(stays))
    def _():
        remote(wsum.at[high], wout.at[high], so_send.at[4], so_recv.at[4], swap_from).start()

    @pl.when(stays)
    def _():
        pltpu.make_async_copy(wsum.at[high], wout.at[high], so_recv.at[4]).start()

    @pl.when(mine != me)
    def _():
        where = {"dp_0": mine // NC, "dp_1": lax.rem(mine, NC)}
        for k, (src, dst) in enumerate(first):
            remote(src, dst, so_send.at[k], so_recv.at[k], where).start()

    @pl.when(mine == me)
    def _():
        for k, (src, dst) in enumerate(first):
            pltpu.make_async_copy(src, dst, so_recv.at[k]).start()

    for n in (4, 5):
        row_sums(n)
    for n in (2, 3, 4, 5):
        finish(n)
    for n in (6, 7):
        row_sums(n)
    finish_gain()

    wait(wmid, so_recv.at[0])
    wait(bmid, so_recv.at[1])

    @pl.when(me != 0)
    def _():
        for k, (src, dst) in enumerate(second):
            remote(src, dst, so_send.at[2 + k], so_recv.at[2 + k], {"sp_0": lax.rem(z + NZ - shift, NZ)}).start()

    @pl.when(me == 0)
    def _():
        for k, (src, dst) in enumerate(second):
            pltpu.make_async_copy(src, dst, so_recv.at[2 + k]).start()

    for n in (1, 0):
        row_sums(n)

    @pl.loop(0, ROWS // 16)
    def _(t):
        rows = pl.ds(pl.multiple_of(t * 16, 16), 16)
        scale = inv[rows, :]
        mean = jnp.sum(dot[rows, :], axis=1, keepdims=True) / WIDTH
        cube = scale * scale * scale * mean
        for g in range(NI * NY):
            at = slice(g * DIM, (g + 1) * DIM)
            scaled = B[0, g // NY, g % NY, rows, :].astype(F32) * gain[0:1, at]
            grad = (scale * scaled - cube * act[rows, at]) * sv[rows, at]
            valg[rows, at] = grad.astype(BF16)

    for n in (6, 7, 1, 0):
        finish(n)

    wait(gy, gn_recv.at[2])
    for i in range(NI):
        for k in range(NY):
            gall[i * NY + k : i * NY + k + 1, :] = gy[k, i : i + 1, :]
    wait(wout.at[low], so_recv.at[2])
    wait(wout.at[high], so_recv.at[4])
    wait(bout, so_recv.at[3])

    wait(X.at[pl.ds(0, NI - 1)], xo_send)
    wait(X.at[:, pl.ds(0, NY - 1)], yo_send)
    wait(S.at[1, :, pl.ds(0, NY - 1)], vy_send)
    wait(V.at[pl.ds(0, NI - 1)], vx_send)
    wait(R0.at[:, pl.ds(0, NY - 1)], yr_send)
    wait(B.at[0, pl.ds(0, NI - 1)], xr_send)
    wait(H1.at[pl.ds(0, NI - 1)], mx_send)
    wait(B.at[1, :, pl.ds(0, NY - 1)], my_send)
    wait(W.at[pl.ds(0, NZ - 1)], wz_send)
    wait(ws.at[pl.ds(0, NZ - 1)], gr_send)
    wait(bsend.at[pl.ds(0, NZ - 1)], bi_send)
    wait(gz.at[pl.ds(0, NZ - 1)], gn_send.at[0])
    wait(gx.at[pl.ds(0, NI - 1)], gn_send.at[1])
    wait(gy.at[pl.ds(0, NY - 1)], gn_send.at[2])

    @pl.when(jnp.logical_not(stays))
    def _():
        for k, (src, dst) in enumerate(moves):
            wait(src, sw_send.at[k])
        wait(wsum.at[high], so_send.at[4])

    @pl.when(mine != me)
    def _():
        for k, (src, dst) in enumerate(first):
            wait(src, so_send.at[k])

    @pl.when(me != 0)
    def _():
        for k, (src, dst) in enumerate(second):
            wait(src, so_send.at[2 + k])


def shards(cotangent, up_pre, value_pre, spatial_weight, spatial_bias, value_gain):
    vmem, dma = pltpu.VMEM, pltpu.SemaphoreType.DMA
    tok = (ROWS, WIDTH)
    out = pl.pallas_call(
        kernel,
        name="gating_backward",
        out_shape=(
            vmem(tok, BF16),
            vmem(tok, BF16),
            vmem((PART, BLOCK), BF16),
            vmem((8, DIM), F32),
            vmem((NY * NI, DIM), F32),
        ),
        in_specs=[pl.BlockSpec(memory_space=pl.ANY)] * 6,
        out_specs=[pl.BlockSpec(memory_space=pltpu.VMEM)] * 5,
        scratch_shapes=[
            vmem(tok, BF16), vmem(tok, BF16), vmem(tok, BF16),
            vmem((PART, BLOCK), BF16), vmem((1, BLOCK), F32), vmem((1, WIDTH), F32),
            vmem((2, NI, NY, ROWS, DIM), BF16),
            vmem((NI, NY, ROWS, DIM), BF16),
            vmem((NI, BLOCK, DIM), BF16),
            vmem((2, BLOCK, NI * DIM), BF16),
            vmem((NX, NY, NC, ROWS, DIM), BF16), vmem((NI, NY, ROWS, DIM), BF16),
            vmem((NX, NY, NC, ROWS, DIM), BF16), vmem((NI, NY, ROWS, DIM), BF16),
            vmem((2, NI, NY, ROWS, DIM), BF16),
            vmem((PART, BLOCK), BF16), vmem((1, BLOCK), F32),
            vmem((NZ, PART, BLOCK), BF16), vmem((BLOCK, BLOCK), BF16), vmem((BLOCK, DIM), F32),
            vmem((NZ, PART, BLOCK), BF16), vmem((4, PART, BLOCK), BF16),
            vmem((2, PART, BLOCK), BF16), vmem((2, PART // 2, BLOCK), BF16),
            vmem((PART, BLOCK), BF16), vmem((PART // 2, BLOCK), BF16),
            vmem((NZ, 8, DIM), F32), vmem((NZ, 8, DIM), F32), vmem((8, BLOCK), F32),
            vmem((8, DIM), F32),
            vmem((8, DIM), F32), vmem((NZ, 8, DIM), F32), vmem((8, DIM), F32), vmem((NI, 8, DIM), F32),
            vmem((NI, DIM), F32), vmem((NY, NI, DIM), F32),
            vmem(tok, F32), vmem(tok, F32), vmem(tok, F32),
            vmem((ROWS, DIM), F32), vmem((ROWS, DIM), F32), vmem((8, DIM), F32),
            dma((6,)),
            dma(()), dma((NI,)), dma(()), dma(()), dma(()), dma(()), dma(()), dma((NX,)),
            dma((2,)), dma((2,)), dma(()), dma((9,)),
            dma(()), dma((NX,)), dma(()), dma((NI,)), dma(()), dma((NI,)), dma(()), dma((NI,)),
            dma(()), dma((8,)), dma(()), dma(()), dma((5,)), dma((5,)),
            dma((3,)), dma((3,)),
        ],
        compiler_params=pltpu.CompilerParams(
            collective_id=0, has_side_effects=True, vmem_limit_bytes=58 * 2**20
        ),
    )(
        cotangent[0], up_pre[0], value_pre[0], spatial_weight[0], spatial_bias, value_gain[None]
    )
    up_grad, value_grad, weight_grad, bias_grad, gain_grad = out
    return up_grad[None], value_grad[None], weight_grad[None].astype(F32), bias_grad[:1], gain_grad.reshape(WIDTH)


def solution(mesh):
    torus = Mesh(mesh.devices.reshape(NZ, NY, NX, NC), ("sp_0", "sp_1", "dp_0", "dp_1"))
    in_specs = (
        P(DP, SP, None),
        P(DP, SP, None),
        P(DP, SP, None),
        P(SP, DP, None),
        P(SP, None),
        P(),
    )
    out_specs = (P(DP, SP, None), P(DP, SP, None), P(SP, DP, None), P(SP, DP), P())
    return jax.shard_map(
        shards, mesh=torus, in_specs=in_specs, out_specs=out_specs, check_vma=False
    )
```

```python
import math

import jax
import jax.numpy as jnp
from jax import lax
from jax.experimental import pallas as pl
from jax.experimental.pallas import tpu as pltpu
from jax.sharding import Mesh
from jax.sharding import PartitionSpec as P

SP = ("sp_0", "sp_1")
DP = ("dp_0", "dp_1")

NZ, NY, NX, NC = 8, 4, 4, 2
NI = NX * NC
ROWS = 256
DIM = 128
WIDTH = NI * NY * DIM
CHUNK = NY * DIM
BLOCK = NY * ROWS
PART = BLOCK // NZ
F32, BF16 = jnp.float32, jnp.bfloat16

norm_floor = 0.5
root_half = 1.0 / math.sqrt(2.0)
inv_root_tau = 1.0 / math.sqrt(2.0 * math.pi)

ORDER = ((0, 0), (0, 1), (1, 0), (3, 0), (1, 1), (3, 1), (2, 0), (2, 1))
NT = (((1,), (1,)), ((), ()))


def phi(x):
    return 0.5 * (1.0 + lax.erf(x * root_half))


def slope(x):
    return phi(x) + x * jnp.exp(-0.5 * x * x) * inv_root_tau


def kernel(
    cot_hbm, up_hbm, val_hbm, w_hbm, bias_hbm, gain_hbm,
    upg, valg, wout, bout, gall,
    cot, up, val, w_own, b_own, gain,
    S, X, V, Y, R0, R1, H0, H1, B,
    w_in, b_in, W, WT, bcol,
    ws, wr, far3, far4, wsum, wmid, bsend, br, bsum, bmid,
    gsend, gz, gxs, gx, gys, gy,
    act, su, sv, inv, dot, gacc,
    in_sem,
    xo_send, xo_recv, yo_send, yo_recv, vy_send, vy_recv, vx_send, vx_recv,
    sw_send, sw_recv, wz_send, wz_recv,
    yr_send, yr_recv, xr_send, xr_recv, mx_send, mx_recv, my_send, my_recv,
    gr_send, gr_recv, bi_send, bi_recv, so_send, so_recv,
    gn_send, gn_recv,
):
    z, y, x, c = (lax.axis_index(a) for a in ("sp_0", "sp_1", "dp_0", "dp_1"))
    me = x * NC + c

    def remote(src, dst, send, recv, where):
        return pltpu.make_async_remote_copy(
            src_ref=src, dst_ref=dst, send_sem=send, recv_sem=recv,
            device_id=where, device_id_type=pl.DeviceIdType.MESH,
        )

    def at_xc(dx, dc):
        return lax.rem(x + dx, NX), lax.rem(c + dc, NC)

    def from_xc(dx, dc):
        return lax.rem(x + NX - dx, NX), lax.rem(c + NC - dc, NC)

    def wait(ref, sem):
        pltpu.make_async_copy(ref, ref, sem).wait()

    loads = [
        pltpu.make_async_copy(src, dst, in_sem.at[k])
        for k, (src, dst) in enumerate(
            ((up_hbm, up), (cot_hbm, cot), (w_hbm, w_own), (bias_hbm, b_own), (val_hbm, val), (gain_hbm, gain))
        )
    ]
    for k in (4, 5, 2, 3, 0, 1):
        loads[k].start()

    barrier = pltpu.get_barrier_semaphore()

    def greet(where):
        pl.semaphore_signal(barrier, inc=1, device_id=where, device_id_type=pl.DeviceIdType.MESH)

    for dx, dc in ORDER[1:]:
        xi, ci = at_xc(dx, dc)
        greet({"dp_0": xi, "dp_1": ci})
    for dy in range(1, NY):
        greet({"sp_1": lax.rem(y + dy, NY)})
    for dz in range(1, NZ):
        greet({"sp_0": lax.rem(z + dz, NZ)})
    shift = x + c * NX
    swap_to = {"sp_0": lax.rem(z + shift, NZ), "dp_0": z // NC, "dp_1": lax.rem(z, NC)}
    turn = lax.rem(z + NZ - me, NZ)

    def part_of(dz):
        t = lax.rem(turn + dz, NZ)
        return lax.rem(t, NX) * NC + t // NX

    mine = part_of(0)
    swap_from = {"sp_0": me, "dp_0": mine // NC, "dp_1": lax.rem(mine, NC)}
    stays = me + z == 0

    @pl.when(jnp.logical_not(stays))
    def _():
        greet(swap_from)
        greet(swap_to)

    def cols(i):
        return pl.ds(pl.multiple_of(i * CHUNK, CHUNK), CHUNK)

    def gate_chunk(i):
        @pl.loop(0, ROWS // 32)
        def _(t):
            rows = pl.ds(pl.multiple_of(t * 32, 32), 32)
            u = up[rows, cols(i)].astype(F32)
            u = (u * phi(u)).astype(BF16).astype(F32)
            g = (cot[rows, cols(i)].astype(F32) * u).astype(BF16)
            for k in range(NY):
                S[0, i, k, rows, :] = g[:, k * DIM : (k + 1) * DIM]

    def span(k, n):
        return pl.ds(pl.multiple_of(k * n, n), n)

    def forward(n):
        xs, cs = from_xc(*ORDER[n])
        s = xs * NC + cs
        src = S.at[0, s] if n == 0 else X.at[s]
        dst = Y.at[0, span(y, ROWS), span(s, DIM)]
        for dy in range(1, NY):
            to = lax.rem(y + dy, NY)
            remote(src.at[to], dst, yo_send, yo_recv, {"sp_1": to}).start()
        pltpu.make_async_copy(src.at[y], dst, yo_recv).start()

    def push(n):
        xi, ci = at_xc(*ORDER[n])
        remote(
            S.at[0, xi * NC + ci], X.at[me], xo_send, xo_recv.at[n], {"dp_0": xi, "dp_1": ci}
        ).start()

    def relay(n):
        xs, cs = from_xc(*ORDER[n])
        wait(X.at[xs * NC + cs], xo_recv.at[n])
        forward(n)

    loads[4].wait()
    loads[5].wait()

    @pl.loop(0, ROWS // 16)
    def _(t):
        rows = pl.ds(pl.multiple_of(t * 16, 16), 16)
        total = jnp.zeros((16, DIM), F32)
        for i in range(NI):
            v = val[rows, i * CHUNK : (i + 1) * CHUNK].astype(F32)
            v = v * phi(v)
            act[rows, i * CHUNK : (i + 1) * CHUNK] = v
            v = v * v
            for k in range(NY):
                total += v[:, k * DIM : (k + 1) * DIM]
        scale = lax.rsqrt(jnp.sum(total, axis=1, keepdims=True) / WIDTH + norm_floor)
        inv[rows, :] = jnp.broadcast_to(scale, (16, DIM))
        for i in range(NI):
            for k in range(NY):
                at = slice((i * NY + k) * DIM, (i * NY + k + 1) * DIM)
                S[1, i, k, rows, :] = (act[rows, at] * scale * gain[0:1, at]).astype(BF16)

    peers = NI - 1 + NY - 1 + NZ - 1

    @pl.when(jnp.logical_not(stays))
    def _():
        pl.semaphore_wait(barrier, peers + 2)

    @pl.when(stays)
    def _():
        pl.semaphore_wait(barrier, peers)

    loads[2].wait()
    loads[3].wait()
    moves = ((w_own, w_in), (b_own, b_in))

    def quarters(src, dst, send, recv, where):
        for k in range(4):
            rows = pl.ds(k * (PART // 4), PART // 4)
            remote(src.at[rows], dst.at[rows], send, recv, where).start()

    @pl.when(jnp.logical_not(stays))
    def _():
        quarters(w_own, w_in, sw_send.at[0], sw_recv.at[0], swap_to)
        remote(b_own, b_in, sw_send.at[1], sw_recv.at[1], swap_to).start()

    @pl.when(stays)
    def _():
        for k, (src, dst) in enumerate(moves):
            pltpu.make_async_copy(src, dst, sw_recv.at[k]).start()

    def of_chip(dx):
        return pl.ds(lax.rem(x + dx, NX) * NC, NC)

    for dx in (1, 3, 2, 0):
        for dy in range(1, NY):
            to = lax.rem(y + dy, NY)
            remote(
                S.at[1, of_chip(dx), to], V.at[of_chip(dx), span(y, ROWS)],
                vy_send, vy_recv.at[dx], {"sp_1": to},
            ).start()
        pltpu.make_async_copy(
            S.at[1, of_chip(dx), y], V.at[of_chip(dx), span(y, ROWS)], vy_recv.at[dx]
        ).start()

    loads[0].wait()
    loads[1].wait()
    for n, d in enumerate(ORDER):
        xi, ci = at_xc(*d)
        gate_chunk(xi * NC + ci)
        if n > 1:
            push(n - 1)
    push(NI - 1)

    def slopes(src, dst):
        @pl.loop(0, ROWS // 32 * NI)
        def _(t):
            rows = pl.ds(pl.multiple_of(t // NI * 32, 32), 32)
            at = cols(lax.rem(t, NI))
            dst[rows, at] = slope(src[rows, at].astype(F32))

    slopes(up, su)

    def along(dz):
        return lax.rem(z + dz, NZ)

    half = PART // 2
    low, high = pl.ds(0, half), pl.ds(half, half)
    wait(w_in, sw_recv.at[0])
    wait(b_in, sw_recv.at[1])
    for dz in (1, 7, 2, 6):
        remote(w_in, W.at[mine], wz_send, wz_recv.at[dz], {"sp_0": along(dz)}).start()
    pltpu.make_async_copy(w_in, W.at[mine], wz_recv.at[0]).start()

    for k in range(BLOCK // DIM):
        part = jnp.broadcast_to(b_in[0:1, k * DIM : (k + 1) * DIM], (DIM, DIM))
        bcol[k * DIM : (k + 1) * DIM, :] = jnp.transpose(part)

    slopes(val, sv)

    for dx in (1, 3, 2, 0):
        wait(V.at[of_chip(dx)], vy_recv.at[dx])
        for dc in range(NC):
            xi, ci = at_xc(dx, dc)
            dst = Y.at[1, :, span(me, DIM)]
            if dx + dc == 0:
                pltpu.make_async_copy(V.at[me], dst, vx_recv.at[0]).start()
            else:
                remote(
                    V.at[xi * NC + ci], dst, vx_send, vx_recv.at[dx], {"dp_0": xi, "dp_1": ci}
                ).start()
    for n in (2, 3, 4, 5):
        relay(n)
    forward(0)
    for n in (1, 6, 7):
        relay(n)

    def pair(dx):
        return lax.rem(x + NX - dx, NX)

    def tile(t):
        return span(t, ROWS)

    for dz, on, full, part, rows in ((6, 1, 3, 4, low), (2, 7, 5, 8, high)):
        kept = part_of(dz)
        wait(W.at[kept], wz_recv.at[NZ - dz])
        remote(W.at[kept], W.at[kept], wz_send, wz_recv.at[full], {"sp_0": along(on)}).start()
        remote(
            W.at[kept, rows], W.at[kept, rows], wz_send, wz_recv.at[part], {"sp_0": along(NZ - dz)}
        ).start()

    for dz, sem in ((0, 0), (7, 1), (1, 7), (5, 3), (3, 5)):
        wait(W.at[part_of(dz)], wz_recv.at[sem])
    wait(W.at[part_of(4), low], wz_recv.at[4])
    wait(W.at[part_of(4), high], wz_recv.at[8])

    def back(dx):
        xs = pair(dx)

        @pl.loop(0, NY)
        def _(t):
            part = jnp.dot(WT[tile(t), :], Y[0, :, span(xs, NC * DIM)], preferred_element_type=F32)
            part = part.astype(BF16)
            R0[xs, t, 0] = part[:, :DIM]
            R0[xs, t, 1] = part[:, DIM:]

        for dy in range(1, NY):
            to = lax.rem(y + dy, NY)
            remote(R0.at[xs, to], H0.at[xs, y], yr_send, yr_recv.at[dx], {"sp_1": to}).start()
        pltpu.make_async_copy(R0.at[xs, y], H0.at[xs, y], yr_recv.at[dx]).start()

    def home(dx):
        xs = pair(dx)
        wait(H0.at[xs], yr_recv.at[dx])
        for dc in range(NC):
            n = ORDER.index(((NX - dx) % NX, dc))
            cs = lax.rem(c + dc, NC)
            src, dst = H0.at[xs, :, cs], B.at[0, me]
            if n == 0:
                pltpu.make_async_copy(src, dst, xr_recv.at[n]).start()
            else:
                remote(src, dst, xr_send, xr_recv.at[n], {"dp_0": xs, "dp_1": cs}).start()

    def mixed(dx):
        xs = pair(dx)

        @pl.loop(0, NY)
        def _(t):
            rows = jnp.concatenate([W[t * 2], W[t * 2 + 1]], axis=0)
            part = jnp.dot(rows, Y[1, :, span(xs, NC * DIM)], preferred_element_type=F32)
            col = bcol[tile(t), :]
            part = (part + jnp.concatenate([col, col], axis=1)).astype(BF16)
            R1[xs * NC, t] = part[:, :DIM]
            R1[xs * NC + 1, t] = part[:, DIM:]

        for dc in range(NC):
            n = ORDER.index(((NX - dx) % NX, dc))
            cs = lax.rem(c + dc, NC)
            if n > 0:
                remote(
                    R1.at[xs * NC + cs], H1.at[me], mx_send, mx_recv.at[n], {"dp_0": xs, "dp_1": cs}
                ).start()

    def settle(n):
        xs, cs = from_xc(*ORDER[n])
        s = xs * NC + cs
        if n > 0:
            wait(H1.at[s], mx_recv.at[n])
        src = (R1 if n == 0 else H1).at[s]
        for dy in range(1, NY):
            to = lax.rem(y + dy, NY)
            remote(src.at[to], B.at[1, s, y], my_send, my_recv.at[n], {"sp_1": to}).start()
        pltpu.make_async_copy(src.at[y], B.at[1, s, y], my_recv.at[n]).start()

    def arrived(a, n):
        xs, cs = from_xc(*ORDER[n])
        s = xs * NC + cs
        wait(B.at[a, s], (my_recv if a else xr_recv).at[n])
        return s

    def value_pair(dx):
        wait(Y.at[1, :, span(pair(dx), NC * DIM)], vx_recv.at[dx])

    def outer(p, q):
        p, q = part_of(p), part_of(q)

        @pl.loop(0, NY)
        def _(j):
            rows = jnp.concatenate([Y[0, span(p, PART), :], Y[0, span(q, PART), :]], axis=0)
            total = lax.dot_general(rows, Y[1, tile(j), :], NT, preferred_element_type=F32).astype(BF16)
            ws[p, :, tile(j)] = total[:PART]
            ws[q, :, tile(j)] = total[PART:]

    value_pair(1)
    mixed(1)
    value_pair(3)
    mixed(3)

    @pl.loop(0, NZ)
    def _(j):
        WT[:, pl.ds(pl.multiple_of(j * PART, PART), PART)] = jnp.transpose(W[j])

    wait(Y.at[0], yo_recv)
    back(1)
    value_pair(2)
    value_pair(0)

    outer(3, 5)
    remote(ws.at[part_of(3)], far3.at[0], gr_send, gr_recv.at[0], {"sp_0": along(1)}).start()
    remote(ws.at[part_of(5)], far3.at[1], gr_send, gr_recv.at[1], {"sp_0": along(7)}).start()
    outer(4, 2)
    remote(ws.at[part_of(4), low], far4.at[0], gr_send, gr_recv.at[2], {"sp_0": along(2)}).start()
    remote(ws.at[part_of(4), high], far4.at[1], gr_send, gr_recv.at[3], {"sp_0": along(6)}).start()
    back(3)
    mixed(2)
    back(2)
    outer(6, 1)
    outer(7, 0)
    for k, dz in enumerate((1, 7)):
        remote(ws.at[part_of(dz)], wr.at[k], gr_send, gr_recv.at[4 + k], {"sp_0": along(dz)}).start()

    ones = jnp.ones((8, NI * DIM), BF16)
    bsum[...] = lax.dot_general(ones, Y[0], NT, preferred_element_type=F32)
    for j in range(NZ):
        bsend[j] = bsum[:, j * DIM : (j + 1) * DIM]
    back(0)
    mixed(0)
    for dz in range(1, NZ):
        remote(bsend.at[part_of(dz)], br.at[z], bi_send, bi_recv, {"sp_0": along(dz)}).start()
    pltpu.make_async_copy(bsend.at[mine], br.at[z], bi_recv).start()

    gacc[...] = jnp.zeros_like(gacc)

    @pl.loop(0, NX * NY)
    def _(t):
        xs, k = t // NY, lax.rem(t, NY)
        total = gacc[...]
        for cs in range(NC):
            part = R0[xs, k, cs].astype(F32) * Y[1, tile(k), span(xs * NC + cs, DIM)].astype(F32)
            total += jnp.sum(part.reshape(ROWS // 8, 8, DIM), axis=0)
        gacc[...] = total

    line = jnp.sum(gacc[...], axis=0, keepdims=True) / gain[0:1, span(me * NY + y, DIM)]
    gsend[...] = jnp.broadcast_to(line, (8, DIM))
    for dz in range(1, NZ):
        remote(gsend, gz.at[z], gn_send.at[0], gn_recv.at[0], {"sp_0": along(dz)}).start()
    pltpu.make_async_copy(gsend, gz.at[z], gn_recv.at[0]).start()

    home(1)
    home(3)

    for k, (dz, rows) in enumerate(((2, low), (6, high))):
        wait(far3.at[k], gr_recv.at[k])
        wait(far4.at[k], gr_recv.at[2 + k])
        to = part_of(dz)
        ws[to] = (ws[to].astype(F32) + far3[k].astype(F32)).astype(BF16)
        ws[to, rows] = (ws[to, rows].astype(F32) + far4[k].astype(F32)).astype(BF16)
        remote(ws.at[to], wr.at[2 + k], gr_send, gr_recv.at[6 + k], {"sp_0": along(dz)}).start()

    for dx in (3, 1):
        for dc in range(NC):
            settle(ORDER.index((dx, dc)))
    home(2)

    settle(1)
    settle(0)
    home(0)
    settle(6)
    settle(7)

    wait(gz, gn_recv.at[0])
    gxs[...] = jnp.sum(gz[...], axis=0)
    for n, d in enumerate(ORDER):
        xi, ci = at_xc(*d)
        if n == 0:
            pltpu.make_async_copy(gxs, gx.at[me], gn_recv.at[1]).start()
        else:
            remote(gxs, gx.at[me], gn_send.at[1], gn_recv.at[1], {"dp_0": xi, "dp_1": ci}).start()

    def finish_gain():
        wait(gx, gn_recv.at[1])
        for i in range(NI):
            gys[i : i + 1, :] = gx[i, 0:1, :]
        for dy in range(1, NY):
            remote(gys, gy.at[y], gn_send.at[2], gn_recv.at[2], {"sp_1": lax.rem(y + dy, NY)}).start()
        pltpu.make_async_copy(gys, gy.at[y], gn_recv.at[2]).start()

    def finish(n):
        s = arrived(1, n)

        @pl.loop(0, ROWS // 32)
        def _(t):
            rows = pl.ds(pl.multiple_of(t * 32, 32), 32)
            for k in range(NY):
                at = pl.ds(pl.multiple_of((s * NY + k) * DIM, DIM), DIM)
                mid = (cot[rows, at].astype(F32) * B[1, s, k, rows, :].astype(F32)).astype(BF16)
                upg[rows, at] = (mid.astype(F32) * su[rows, at]).astype(BF16)

    dot[...] = jnp.zeros_like(dot)

    def row_sums(n):
        s = arrived(0, n)

        @pl.loop(0, ROWS // 32)
        def _(t):
            rows = pl.ds(pl.multiple_of(t * 32, 32), 32)
            total = dot[rows, :]
            for k in range(NY):
                at = pl.ds(pl.multiple_of((s * NY + k) * DIM, DIM), DIM)
                total += B[0, s, k, rows, :].astype(F32) * gain[0:1, at] * act[rows, at]
            dot[rows, :] = total

    for n in (2, 3):
        row_sums(n)

    for k in range(4):
        wait(wr.at[k], gr_recv.at[4 + k])
    wait(br, bi_recv)

    @pl.loop(0, PART // 16)
    def _(t):
        rows = pl.ds(pl.multiple_of(t * 16, 16), 16)
        total = ws[mine, rows, :].astype(F32)
        for k in range(4):
            total += wr[k, rows, :].astype(F32)
        wsum[rows, :] = total.astype(BF16)

    bsum[:, :DIM] = jnp.sum(br[...], axis=0)
    some, rest = low, high
    first = ((wsum.at[some], wmid), (bsum.at[:, pl.ds(0, DIM)], bmid))
    second = ((wmid, wout.at[some]), (bmid, bout))

    @pl.when(jnp.logical_not(stays))
    def _():
        remote(wsum.at[rest], wout.at[rest], so_send.at[4], so_recv.at[4], swap_from).start()

    @pl.when(stays)
    def _():
        pltpu.make_async_copy(wsum.at[rest], wout.at[rest], so_recv.at[4]).start()

    @pl.when(mine != me)
    def _():
        where = {"dp_0": mine // NC, "dp_1": lax.rem(mine, NC)}
        for k, (src, dst) in enumerate(first):
            remote(src, dst, so_send.at[k], so_recv.at[k], where).start()

    @pl.when(mine == me)
    def _():
        for k, (src, dst) in enumerate(first):
            pltpu.make_async_copy(src, dst, so_recv.at[k]).start()

    for n in (4, 5):
        row_sums(n)
    for n in (2, 3, 4, 5):
        finish(n)
    for n in (1, 0):
        row_sums(n)
    for n in (1, 0):
        finish(n)
    for n in (6, 7):
        row_sums(n)
    finish_gain()

    wait(wmid, so_recv.at[0])
    wait(bmid, so_recv.at[1])

    @pl.when(me != 0)
    def _():
        for k, (src, dst) in enumerate(second):
            remote(src, dst, so_send.at[2 + k], so_recv.at[2 + k], {"sp_0": lax.rem(z + NZ - shift, NZ)}).start()

    @pl.when(me == 0)
    def _():
        for k, (src, dst) in enumerate(second):
            pltpu.make_async_copy(src, dst, so_recv.at[2 + k]).start()


    @pl.loop(0, ROWS // 16)
    def _(t):
        rows = pl.ds(pl.multiple_of(t * 16, 16), 16)
        scale = inv[rows, :]
        mean = jnp.sum(dot[rows, :], axis=1, keepdims=True) / WIDTH
        cube = scale * scale * scale * mean
        for g in range(NI * NY):
            at = slice(g * DIM, (g + 1) * DIM)
            scaled = B[0, g // NY, g % NY, rows, :].astype(F32) * gain[0:1, at]
            grad = (scale * scaled - cube * act[rows, at]) * sv[rows, at]
            valg[rows, at] = grad.astype(BF16)

    for n in (6, 7):
        finish(n)

    wait(gy, gn_recv.at[2])
    for i in range(NI):
        for k in range(NY):
            gall[i * NY + k : i * NY + k + 1, :] = gy[k, i : i + 1, :]
    wait(wout.at[some], so_recv.at[2])
    wait(wout.at[rest], so_recv.at[4])
    wait(bout, so_recv.at[3])

    wait(X.at[pl.ds(0, NI - 1)], xo_send)
    wait(X.at[:, pl.ds(0, NY - 1)], yo_send)
    wait(S.at[1, :, pl.ds(0, NY - 1)], vy_send)
    wait(V.at[pl.ds(0, NI - 1)], vx_send)
    wait(R0.at[:, pl.ds(0, NY - 1)], yr_send)
    wait(B.at[0, pl.ds(0, NI - 1)], xr_send)
    wait(H1.at[pl.ds(0, NI - 1)], mx_send)
    wait(B.at[1, :, pl.ds(0, NY - 1)], my_send)
    wait(W.at[pl.ds(0, NZ - 1)], wz_send)
    wait(ws.at[pl.ds(0, NZ - 1)], gr_send)
    wait(bsend.at[pl.ds(0, NZ - 1)], bi_send)
    wait(gz.at[pl.ds(0, NZ - 1)], gn_send.at[0])
    wait(gx.at[pl.ds(0, NI - 1)], gn_send.at[1])
    wait(gy.at[pl.ds(0, NY - 1)], gn_send.at[2])

    @pl.when(jnp.logical_not(stays))
    def _():
        for k, (src, dst) in enumerate(moves):
            wait(src, sw_send.at[k])
        wait(wsum.at[rest], so_send.at[4])

    @pl.when(mine != me)
    def _():
        for k, (src, dst) in enumerate(first):
            wait(src, so_send.at[k])

    @pl.when(me != 0)
    def _():
        for k, (src, dst) in enumerate(second):
            wait(src, so_send.at[2 + k])


def shards(cotangent, up_pre, value_pre, spatial_weight, spatial_bias, value_gain):
    vmem, dma = pltpu.VMEM, pltpu.SemaphoreType.DMA
    tok = (ROWS, WIDTH)
    out = pl.pallas_call(
        kernel,
        name="gating_backward",
        out_shape=(
            vmem(tok, BF16),
            vmem(tok, BF16),
            vmem((PART, BLOCK), BF16),
            vmem((8, DIM), F32),
            vmem((NY * NI, DIM), F32),
        ),
        in_specs=[pl.BlockSpec(memory_space=pl.ANY)] * 6,
        out_specs=[pl.BlockSpec(memory_space=pltpu.VMEM)] * 5,
        scratch_shapes=[
            vmem(tok, BF16), vmem(tok, BF16), vmem(tok, BF16),
            vmem((PART, BLOCK), BF16), vmem((1, BLOCK), F32), vmem((1, WIDTH), F32),
            vmem((2, NI, NY, ROWS, DIM), BF16),
            vmem((NI, NY, ROWS, DIM), BF16),
            vmem((NI, BLOCK, DIM), BF16),
            vmem((2, BLOCK, NI * DIM), BF16),
            vmem((NX, NY, NC, ROWS, DIM), BF16), vmem((NI, NY, ROWS, DIM), BF16),
            vmem((NX, NY, NC, ROWS, DIM), BF16), vmem((NI, NY, ROWS, DIM), BF16),
            vmem((2, NI, NY, ROWS, DIM), BF16),
            vmem((PART, BLOCK), BF16), vmem((1, BLOCK), F32),
            vmem((NZ, PART, BLOCK), BF16), vmem((BLOCK, BLOCK), BF16), vmem((BLOCK, DIM), F32),
            vmem((NZ, PART, BLOCK), BF16), vmem((4, PART, BLOCK), BF16),
            vmem((2, PART, BLOCK), BF16), vmem((2, PART // 2, BLOCK), BF16),
            vmem((PART, BLOCK), BF16), vmem((PART // 2, BLOCK), BF16),
            vmem((NZ, 8, DIM), F32), vmem((NZ, 8, DIM), F32), vmem((8, BLOCK), F32),
            vmem((8, DIM), F32),
            vmem((8, DIM), F32), vmem((NZ, 8, DIM), F32), vmem((8, DIM), F32), vmem((NI, 8, DIM), F32),
            vmem((NI, DIM), F32), vmem((NY, NI, DIM), F32),
            vmem(tok, F32), vmem(tok, F32), vmem(tok, F32),
            vmem((ROWS, DIM), F32), vmem((ROWS, DIM), F32), vmem((8, DIM), F32),
            dma((6,)),
            dma(()), dma((NI,)), dma(()), dma(()), dma(()), dma((NX,)), dma(()), dma((NX,)),
            dma((2,)), dma((2,)), dma(()), dma((9,)),
            dma(()), dma((NX,)), dma(()), dma((NI,)), dma(()), dma((NI,)), dma(()), dma((NI,)),
            dma(()), dma((8,)), dma(()), dma(()), dma((5,)), dma((5,)),
            dma((3,)), dma((3,)),
        ],
        compiler_params=pltpu.CompilerParams(
            collective_id=0, has_side_effects=True, vmem_limit_bytes=58 * 2**20
        ),
    )(
        cotangent[0], up_pre[0], value_pre[0], spatial_weight[0], spatial_bias, value_gain[None]
    )
    up_grad, value_grad, weight_grad, bias_grad, gain_grad = out
    return up_grad[None], value_grad[None], weight_grad[None].astype(F32), bias_grad[:1], gain_grad.reshape(WIDTH)


def solution(mesh):
    torus = Mesh(mesh.devices.reshape(NZ, NY, NX, NC), ("sp_0", "sp_1", "dp_0", "dp_1"))
    in_specs = (
        P(DP, SP, None),
        P(DP, SP, None),
        P(DP, SP, None),
        P(SP, DP, None),
        P(SP, None),
        P(),
    )
    out_specs = (P(DP, SP, None), P(DP, SP, None), P(SP, DP, None), P(SP, DP), P())
    return jax.shard_map(
        shards, mesh=torus, in_specs=in_specs, out_specs=out_specs, check_vma=False
    )
```
